256 devices in a mesh: ep: 64 (over z, y, core), tp: 4 (over x).
Axes of the slice: x: 4, y: 4, z: 8, core: 2. Of those that a mesh axis runs over, the one named last changes fastest.
Arguments:
- tokens: bfloat16 [1536, 2048], P('ep'), may hold values from -6 to 6
- norm_attn: float32 [2048], replicated, may hold values from 0.1 to 1.9
- w_query: bfloat16 [2048, 2048], P(None, 'tp'), may hold values from -0.125 to 0.125
- w_key: bfloat16 [2048, 256], P(None, 'tp'), may hold values from -0.125 to 0.125
- w_value: bfloat16 [2048, 256], P(None, 'tp'), may hold values from -0.125 to 0.125
- w_out: bfloat16 [2048, 2048], P('tp'), may hold values from -1 to 1
- head_bias: float32 [32], P('tp'), may hold values from -7 to -3
- key_cache: bfloat16 [1536, 4, 1024, 64], P('ep', 'tp'), may hold values from -6 to 6
- value_cache: bfloat16 [1536, 4, 1024, 64], P('ep', 'tp'), may hold values from -6 to 6
- lengths: int32 [1536], P('ep'), may hold values from 1 to 1024, 786432 in all
- norm_ffn: float32 [2048], replicated, may hold values from 0.1 to 1.9
- w_group: bfloat16 [2048, 4], replicated, may hold values from -0.125 to 0.125
- w_fine: bfloat16 [2048, 64], replicated, may hold values from -0.125 to 0.125
- routes: int32 [1536, 2], P('ep'), may hold values from 0 to 63, as said below
- e_gate: bfloat16 [64, 2048, 512], P('ep', 'tp'), may hold values from -0.125 to 0.125
- e_up: bfloat16 [64, 2048, 512], P('ep', 'tp'), may hold values from -0.125 to 0.125
- e_down: bfloat16 [64, 512, 2048], P('ep', None, 'tp'), may hold values from -1 to 1
- d_gate: bfloat16 [2048, 8192], P('tp', 'ep'), may hold values from -0.125 to 0.125
- d_up: bfloat16 [2048, 8192], P('tp', 'ep'), may hold values from -0.125 to 0.125
- d_down: bfloat16 [8192, 2048], P('ep', 'tp'), may hold values from -0.25 to 0.25
- w_mix: float32 [2048], replicated, may hold values from -0.125 to 0.125
Outputs:
- mixed: bfloat16 [1536, 2048], P('ep', 'tp')
- new_keys: bfloat16 [1536, 4, 64], P('ep', 'tp')
- new_values: bfloat16 [1536, 4, 64], P('ep', 'tp')
The draws below stay inside these ranges and needn't reach their ends.
Inputs may be any that keep to these rules, and one draw needn't show every extreme that they name: `routes`: the 2 experts of a row are distinct and lie in one group of 16 consecutive experts. Among the rows of one device each expert is named at most 2 times. One group, the same on every device, is named by exactly 16 rows of every device, so that each of its experts is named exactly 2 times by every device.
All inputs are finite; a program needn't handle non-finite values. No bound on the sum of `lengths` on one device may be relied on, other than what follows from the above.
Results may differ from the reference program's by a relative error of at most 0.019.
Values may be sent and summed in bfloat16 or wider, within the bound.
No kernel may reach another device: no remote copies, remote signals or barrier semaphores. Data moves between devices by JAX's collectives and lax.ppermute only.
A program may use at most 128 MiB of HBM per device.

```python
import math
import jax
import jax.numpy as jnp
import numpy as np
from jax import lax

D = 2048
HEADS = 32
KV_HEADS = 4
DH = 64
FFE = 512
DENSE_FF = 8192
GROUPS = 4
TOP_K = 2
SEQ_DEV = 24
LEN = 1024
SEQUENCES = 1536
EXPERTS = 64
EPG = 16
FULL_ROWS = 16
SLOTS = 128
N_TP = 4


def draw_routes(key, part):
    blocks = SEQUENCES // SEQ_DEV
    base_key = jax.random.fold_in(key, 11)
    full_key, blocks_key = jax.random.split(base_key)
    full_group = jax.random.randint(full_key, (), 0, GROUPS)

    def one_block(block_seed):
        ranking_key, other_key, tables_key = jax.random.split(block_seed, 3)
        ranking = jax.random.permutation(ranking_key, SEQ_DEV)
        other_group = jax.random.randint(other_key, (SEQ_DEV,), 1, GROUPS)
        group_ids = jnp.where(ranking < FULL_ROWS, full_group, (full_group + other_group) % GROUPS)
        same_group = group_ids[:, None] == group_ids[None, :]
        before = ranking[None, :] < ranking[:, None]
        position = jnp.sum(same_group & before, axis=1)
        tables = jax.vmap(lambda seed_key: jax.random.permutation(seed_key, EPG))(jax.random.split(tables_key, GROUPS))
        chosen = [tables[group_ids, (TOP_K * position + slot_index) % EPG] for slot_index in range(TOP_K)]
        return jnp.stack([group_ids * EPG + member for member in chosen], axis=1)
    result = jax.vmap(one_block)(jax.random.split(blocks_key, blocks))
    return result.reshape(SEQUENCES, TOP_K).astype(jnp.int32)


def shard_levels(rng, extent, pieces, low, top_value):
    loudness, own = 1.0, jax.random.fold_in(rng, 6)
    for dim, shards_of in pieces:
        draws = jnp.exp(jax.random.uniform(jax.random.fold_in(own, dim), (shards_of,), jnp.float32, low / len(pieces), top_value / len(pieces)))
        loudness = loudness * jnp.repeat(draws, extent[dim] // shards_of).reshape([-1 if axis == dim else 1 for axis in range(len(extent))])
    return loudness


def length_profile(number_of, total, reach, lean):
    portions = [(1 << 20) // math.isqrt(grade ** lean) + 1 for grade in range(2, number_of + 1)]
    surplus, counts = total - reach - (number_of - 1), [1] * (number_of - 1)
    while surplus > 0:
        candidates = [i for i in range(number_of - 1) if counts[i] < reach]
        whole, budget = sum([portions[i] for i in candidates]), surplus
        for i in candidates:
            more = min(reach - counts[i], max(1, budget * portions[i] // whole), surplus)
            counts[i] = counts[i] + more
            surplus = surplus - more
    return np.array([reach] + counts)


def uneven(rng, count, total, bound, slope):
    if count == 2:
        one = jax.random.randint(rng, (), max(1, total - bound), min(bound, total - 1) + 1)
        return jnp.stack([one, total - one])
    tallies = jnp.asarray(length_profile(count, total, bound, slope), jnp.int32)
    couples = (count - 1) // 2
    donor, sink = tallies[1:1 + 2 * couples:2], tallies[2:2 + 2 * couples:2]
    room = jnp.minimum(donor - 1, bound - sink)
    moved = jax.random.randint(jax.random.fold_in(rng, 1), (couples,), 0, 1 << 20) % (room + 1)
    tallies = tallies.at[1:1 + 2 * couples:2].set(donor - moved).at[2:2 + 2 * couples:2].set(sink + moved)
    return tallies[jax.random.permutation(jax.random.fold_in(rng, 2), count)]


def noise(key, dims, width, limit, pieces=(), kind=jnp.bfloat16):
    level = shard_levels(key, dims, pieces, -0.22, 0.18) if pieces else 1.0
    entries = jax.random.normal(key, dims, jnp.float32) * width * level
    return jnp.minimum(jnp.maximum(entries, -limit), limit).astype(kind)


def setup_inputs(seed: int = 0) -> dict:
    key_list = jax.random.split(jax.random.key(seed), 22)
    tokens = noise(key_list[0], (SEQUENCES, D), 1.0, 6.0, ((0, 64),))
    norm_attn = jnp.clip(1.0 + 0.18 * jax.random.normal(key_list[1], (D,), jnp.float32), 0.1, 1.9)
    w_query = noise(key_list[2], (D, HEADS * DH), D ** -0.5, 0.125, ((1, 4),))
    w_key = noise(key_list[3], (D, KV_HEADS * DH), D ** -0.5, 0.125, ((1, 4),))
    w_value = noise(key_list[4], (D, KV_HEADS * DH), D ** -0.5, 0.125, ((1, 4),))
    w_out = noise(key_list[5], (HEADS * DH, D), (HEADS * DH // 64) ** -0.5, 1.0, ((0, 4),))
    head_bias = jnp.clip(-7.0 + 4.0 * jax.random.uniform(key_list[6], (HEADS,), jnp.float32) ** shard_levels(key_list[6], (HEADS,), ((0, 4),), -0.2, 0.2), -7.0, -3.0)
    key_cache = noise(key_list[7], (SEQUENCES, KV_HEADS, LEN, DH), 1.0, 6.0, ((0, 64), (1, 4)))
    value_cache = noise(key_list[8], (SEQUENCES, KV_HEADS, LEN, DH), 1.0, 6.0, ((0, 64), (1, 4)))
    lengths = uneven(key_list[9], SEQUENCES, SEQUENCES * LEN // 2, LEN, 2).astype(jnp.int32)
    norm_ffn = jnp.clip(1.0 + 0.18 * jax.random.normal(key_list[10], (D,), jnp.float32), 0.1, 1.9)
    w_group = noise(key_list[11], (D, GROUPS), D ** -0.5, 0.125)
    w_fine = noise(key_list[12], (D, EXPERTS), D ** -0.5, 0.125)
    routes = draw_routes(jax.random.fold_in(key_list[21], 71), 0)
    e_gate = noise(key_list[14], (EXPERTS, D, FFE), D ** -0.5, 0.125, ((0, 64), (1, 4)))
    e_up = noise(key_list[15], (EXPERTS, D, FFE), D ** -0.5, 0.125, ((0, 64), (1, 4)))
    e_down = noise(key_list[16], (EXPERTS, FFE, D), (FFE // 16) ** -0.5, 1.0, ((0, 64), (2, 4)))
    d_gate = noise(key_list[17], (D, DENSE_FF), D ** -0.5, 0.125, ((0, 4), (1, 64)))
    d_up = noise(key_list[18], (D, DENSE_FF), D ** -0.5, 0.125, ((0, 4), (1, 64)))
    d_down = noise(key_list[19], (DENSE_FF, D), (DENSE_FF // 16) ** -0.5, 0.25, ((0, 64), (1, 4)))
    w_mix = noise(key_list[20], (D,), D ** -0.5, 0.125, (), jnp.float32)
    return dict(tokens=tokens, norm_attn=norm_attn, w_query=w_query, w_key=w_key, w_value=w_value, w_out=w_out, head_bias=head_bias, key_cache=key_cache, value_cache=value_cache, lengths=lengths, norm_ffn=norm_ffn, w_group=w_group, w_fine=w_fine, routes=routes, e_gate=e_gate, e_up=e_up, e_down=e_down, d_gate=d_gate, d_up=d_up, d_down=d_down, w_mix=w_mix)


def normed(values, gains):
    wide = values.astype(jnp.float32)
    return wide * lax.rsqrt(lax.optimization_barrier(jnp.mean(wide * wide, axis=-1, keepdims=True)) + 1e-06) * gains

def route_weights(group_logits, fine_logits, chosen, per_group):
    group_iota = lax.iota(jnp.int32, group_logits.shape[1])
    own_group = chosen[:, 0] // per_group
    own_logit = lax.optimization_barrier(jnp.sum(jnp.where(group_iota[None, :] == own_group[:, None], group_logits, 0.0), axis=1))
    group_share = 1.0 / lax.optimization_barrier(jnp.sum(jnp.exp(group_logits - own_logit[:, None]), axis=1))
    expert_iota = lax.iota(jnp.int32, fine_logits.shape[1])
    picked = lax.optimization_barrier(jnp.sum(jnp.where(expert_iota[None, None, :] == chosen[:, :, None], fine_logits[:, None, :], 0.0), axis=2))
    within = 1.0 / lax.optimization_barrier(jnp.sum(jnp.exp(picked[:, None, :] - picked[:, :, None]), axis=2))
    return group_share[:, None] * within

def attend(queries, key_cache, value_cache, lengths, head_bias):
    per_kv = HEADS // KV_HEADS
    query_blocks = queries.reshape(SEQUENCES // SEQ_DEV, SEQ_DEV, KV_HEADS, per_kv, DH)
    key_blocks = key_cache.reshape(SEQUENCES // SEQ_DEV, SEQ_DEV, KV_HEADS, LEN, DH)
    value_blocks = value_cache.reshape(SEQUENCES // SEQ_DEV, SEQ_DEV, KV_HEADS, LEN, DH)
    length_blocks = lengths.reshape(SEQUENCES // SEQ_DEV, SEQ_DEV)
    bias_table = head_bias.reshape(KV_HEADS, per_kv).astype(jnp.float32)

    def one_block(stacked):
        queries_b, keys_b, values_b, counts_b = stacked
        scores = jnp.einsum('bkgd,bksd->bkgs', queries_b.astype(jnp.float32), keys_b.astype(jnp.float32))
        scores = scores * DH ** (-0.5) + bias_table[None, :, :, None]
        positions = jnp.arange(LEN, dtype=jnp.int32)
        inside = (positions[None, :] < counts_b[:, None])[:, None, None, :]
        fails = jnp.where(inside, jax.nn.log_sigmoid(-scores), 0.0)
        between = lax.cumsum(fails, axis=3, reverse=True) - fails
        weights = jnp.where(inside, jnp.exp(jax.nn.log_sigmoid(scores) + between), 0.0).astype(jnp.bfloat16)
        mixed_b = jnp.einsum('bkgs,bksd->bkgd', weights.astype(jnp.float32), values_b.astype(jnp.float32))
        return mixed_b.astype(jnp.bfloat16)
    result = lax.map(one_block, (query_blocks, key_blocks, value_blocks, length_blocks))
    return result.reshape(SEQUENCES, HEADS * DH)

def reference(tokens, norm_attn, w_query, w_key, w_value, w_out, head_bias, key_cache, value_cache, lengths, norm_ffn, w_group, w_fine, routes, e_gate, e_up, e_down, d_gate, d_up, d_down, w_mix):
    h_first = normed(tokens, norm_attn).astype(jnp.bfloat16)
    queries = jnp.dot(h_first, w_query, preferred_element_type=jnp.float32).astype(jnp.bfloat16)
    new_keys = jnp.dot(h_first, w_key, preferred_element_type=jnp.float32).astype(jnp.bfloat16)
    new_values = jnp.dot(h_first, w_value, preferred_element_type=jnp.float32).astype(jnp.bfloat16)
    heads_out = attend(queries, key_cache, value_cache, lengths, head_bias)
    per_tp = HEADS * DH // N_TP
    attended = jnp.zeros((SEQUENCES, D), jnp.float32)
    for block_index in range(N_TP):
        piece = jnp.dot(heads_out[:, block_index * per_tp:(block_index + 1) * per_tp], w_out[block_index * per_tp:(block_index + 1) * per_tp], preferred_element_type=jnp.float32).astype(jnp.bfloat16)
        attended = attended + lax.optimization_barrier(piece).astype(jnp.float32)
    resid = tokens.astype(jnp.float32) + attended
    h_second = normed(resid, norm_ffn).astype(jnp.bfloat16)
    group_logits = jnp.dot(h_second, w_group, preferred_element_type=jnp.float32)
    fine_logits = jnp.dot(h_second, w_fine, preferred_element_type=jnp.float32)
    shares = route_weights(group_logits, fine_logits, routes, EPG)

    def expert_step(totals, stacked):
        gate_w, up_w, down_w, number = stacked
        names_it = routes == number
        is_hit = jnp.any(names_it, axis=1)
        expert_share = lax.optimization_barrier(jnp.sum(jnp.where(names_it, shares, 0.0), axis=1))
        row_index = jnp.nonzero(is_hit, size=SLOTS, fill_value=0)[0].astype(jnp.int32)
        is_valid = (jnp.arange(SLOTS, dtype=jnp.int32) < jnp.sum(is_hit.astype(jnp.int32))).astype(jnp.float32)
        picked_rows = h_second[row_index]
        gate_pre = jnp.dot(picked_rows, gate_w, preferred_element_type=jnp.float32)
        up_pre = jnp.dot(picked_rows, up_w, preferred_element_type=jnp.float32)
        hidden = (jax.nn.silu(gate_pre) * up_pre).astype(jnp.bfloat16)
        expert_out = jnp.dot(hidden, down_w, preferred_element_type=jnp.float32).astype(jnp.bfloat16)
        scaled = expert_out.astype(jnp.float32) * (expert_share[row_index] * is_valid)[:, None]
        return (totals.at[row_index].add(scaled), None)
    moe, _ = lax.scan(expert_step, jnp.zeros((SEQUENCES, D), jnp.float32), (e_gate, e_up, e_down, jnp.arange(EXPERTS, dtype=jnp.int32)))
    dense_gate = jnp.dot(h_second, d_gate, preferred_element_type=jnp.float32)
    dense_up = jnp.dot(h_second, d_up, preferred_element_type=jnp.float32)
    dense_hidden = (jax.nn.silu(dense_gate) * dense_up).astype(jnp.bfloat16)
    dense = jnp.dot(dense_hidden, d_down, preferred_element_type=jnp.float32)
    mix_gate = jax.nn.sigmoid(jnp.dot(h_second.astype(jnp.float32), w_mix, precision=lax.Precision.HIGHEST))
    mixed = (resid + moe + mix_gate[:, None] * dense).astype(jnp.bfloat16)
    return (mixed, new_keys.reshape(SEQUENCES, KV_HEADS, DH), new_values.reshape(SEQUENCES, KV_HEADS, DH))
```

```python
import functools

import jax
import jax.numpy as jnp
from jax import lax
from jax.experimental import pallas as pl
from jax.experimental.pallas import tpu as pltpu
from jax.sharding import Mesh
from jax.sharding import PartitionSpec as P

GROUPS = 4
TOP_K = 2
EP = ("ep_0", "ep_1", "ep_2")
Z, Y, CORE, TP = "ep_0", "ep_1", "ep_2", "tp"

norm_eps = 1e-06
segment_len = 128
NT = (((1,), (1,)), ((), ()))


def shifted(x, axis, step):
    size = lax.axis_size(axis)
    return lax.ppermute(x, axis, [(i, (i + step) % size) for i in range(size)])


def normed(values, gains):
    wide = values.astype(jnp.float32)
    return wide * lax.rsqrt(jnp.mean(wide * wide, axis=-1, keepdims=True) + norm_eps) * gains


def suffix_sums(terms):
    length = terms.shape[-1]
    pieces = length // segment_len
    shaped = terms.reshape(terms.shape[:-1] + (pieces, segment_len))
    inner = lax.iota(jnp.int32, segment_len)
    later_inner = (inner[:, None] > inner[None, :]).astype(jnp.float32)
    within = jnp.einsum("...ij,jk->...ik", shaped, later_inner, precision=lax.Precision.HIGHEST)
    outer = lax.iota(jnp.int32, pieces)
    later_outer = (outer[:, None] > outer[None, :]).astype(jnp.float32)
    carried = jnp.einsum(
        "...i,ij->...j", jnp.sum(shaped, axis=-1), later_outer, precision=lax.Precision.HIGHEST
    )
    return (within + carried[..., None]).reshape(terms.shape)


def stick_read(queries, keys, values, lengths, bias_table):
    scores = jnp.einsum("bkgd,bksd->bkgs", queries, keys, preferred_element_type=jnp.float32)
    scores = scores * queries.shape[-1] ** (-0.5) + bias_table[None, :, :, None]
    positions = lax.iota(jnp.int32, keys.shape[2])
    inside = (positions[None, :] < lengths[:, None])[:, None, None, :]
    fails = jnp.where(inside, jax.nn.log_sigmoid(-scores), 0.0)
    weights = jnp.where(inside, jnp.exp(jax.nn.log_sigmoid(scores) + suffix_sums(fails)), 0.0)
    result = jnp.einsum(
        "bkgs,bksd->bkgd", weights.astype(jnp.bfloat16), values, preferred_element_type=jnp.float32
    )
    return result.astype(jnp.bfloat16).reshape(queries.shape[0], -1)


def route_weights(group_logits, fine_logits, chosen, per_group):
    group_iota = lax.iota(jnp.int32, group_logits.shape[1])
    own_group = chosen[:, 0] // per_group
    own_logit = jnp.sum(
        jnp.where(group_iota[None, :] == own_group[:, None], group_logits, 0.0), axis=1
    )
    group_share = 1.0 / jnp.sum(jnp.exp(group_logits - own_logit[:, None]), axis=1)
    expert_iota = lax.iota(jnp.int32, fine_logits.shape[1])
    picked = jnp.sum(
        jnp.where(expert_iota[None, None, :] == chosen[:, :, None], fine_logits[:, None, :], 0.0),
        axis=2,
    )
    within = 1.0 / jnp.sum(jnp.exp(picked[:, None, :] - picked[:, :, None]), axis=2)
    return group_share[:, None] * within


def slot_ranks(flat_routes):
    count = flat_routes.shape[0]
    same_expert = flat_routes[:, None] == flat_routes[None, :]
    position = lax.iota(jnp.int32, count)
    earlier = position[None, :] < position[:, None]
    return jnp.sum(same_expert & earlier, axis=1)


def silu(v):
    return v / (1.0 + jnp.exp(-v))


def dense_kernel(here_ref, there_ref, *refs):
    blocks, out_ref = refs[:-1], refs[-1]
    units = blocks[0].shape[0] // 3
    cut = [
        jnp.concatenate([b[part * units : (part + 1) * units, :] for b in blocks], axis=0)
        for part in range(3)
    ]
    rows = jnp.concatenate([here_ref[...], there_ref[...]], axis=0)
    gate = lax.dot_general(rows, cut[0], NT, preferred_element_type=jnp.float32)
    up = lax.dot_general(rows, cut[1], NT, preferred_element_type=jnp.float32)
    hidden = (silu(gate) * up).astype(jnp.bfloat16)
    seq, width = out_ref.shape[1], out_ref.shape[2]
    y, c = lax.axis_index(Y), lax.axis_index(CORE)
    ys, tps = lax.axis_size(Y), lax.axis_size(TP)
    for t in range(tps):
        part = jnp.dot(
            hidden, cut[2][:, t * width : (t + 1) * width], preferred_element_type=jnp.float32
        )
        for other in range(2):
            core = c if other == 0 else 1 - c
            for k in range(ys):
                owner = (lax.rem(y - k + ys, ys) * 2 + core) * tps + t
                at = (other * ys + k) * seq
                out_ref[owner] = part[at : at + seq].astype(jnp.bfloat16)


def dense_parts(here, there, blocks, seq, width):
    members = lax.axis_size(Y) * lax.axis_size(CORE) * lax.axis_size(TP)
    return pl.pallas_call(
        dense_kernel,
        out_shape=jax.ShapeDtypeStruct((members, seq, width), jnp.bfloat16),
        cost_estimate=pl.CostEstimate(
            flops=1_300_000_000, bytes_accessed=5_000_000, transcendentals=50_000
        ),
        name="dense_parts",
    )(here, there, *blocks)


def expert_in_kernel(rows_ref, gate_ref, up_ref, out_ref):
    t, tps = lax.axis_index(TP), lax.axis_size(TP)
    width = out_ref.shape[2] // 2
    rows = rows_ref[...]
    for u in range(tps):
        at = slice(u * width, (u + 1) * width)
        both = jnp.concatenate([gate_ref[:, at], up_ref[:, at]], axis=1)
        pre = jnp.dot(rows, both, preferred_element_type=jnp.float32)
        out_ref[lax.rem(u - t + tps, tps)] = pre.astype(jnp.bfloat16)


def expert_in(rows, gate, up):
    tps = lax.axis_size(TP)
    return pl.pallas_call(
        expert_in_kernel,
        out_shape=jax.ShapeDtypeStruct(
            (tps, rows.shape[0], 2 * gate.shape[1] // tps), jnp.bfloat16
        ),
        cost_estimate=pl.CostEstimate(
            flops=140_000_000, bytes_accessed=1_400_000, transcendentals=0
        ),
        name="expert_in",
    )(rows, gate, up)


def expert_out_kernel(*refs):
    hiddens, down_ref, out_ref = refs[:-2], refs[-2], refs[-1]
    t, tps = lax.axis_index(TP), lax.axis_size(TP)
    units = hiddens[0].shape[1]
    total = None
    for k in range(tps):
        at = pl.multiple_of(lax.rem(t - k + tps, tps) * units, units)
        term = jnp.dot(
            hiddens[k][...], down_ref[pl.ds(at, units), :], preferred_element_type=jnp.float32
        )
        total = term if total is None else total + term
    out_ref[...] = total.astype(jnp.bfloat16)


def expert_out(hiddens, down):
    return pl.pallas_call(
        expert_out_kernel,
        out_shape=jax.ShapeDtypeStruct((hiddens[0].shape[0], down.shape[1]), jnp.bfloat16),
        cost_estimate=pl.CostEstimate(
            flops=70_000_000, bytes_accessed=800_000, transcendentals=0
        ),
        name="expert_out",
    )(*hiddens, down)


def dense_weights(d_gate, d_up, d_down):
    tps = lax.axis_size(TP)
    width, units = d_gate.shape
    piece = units // tps
    outgoing = jnp.concatenate(
        [
            d_gate.T.reshape(tps, piece, width),
            d_up.T.reshape(tps, piece, width),
            d_down.reshape(tps, piece, width),
        ],
        axis=1,
    )
    arrived = lax.all_to_all(outgoing, TP, split_axis=0, concat_axis=0, tiled=True)
    own = arrived.transpose(1, 0, 2).reshape(3 * piece, tps * width)
    blocks = [own]
    right = left = own
    for step in range(lax.axis_size(Z) // 2):
        right = shifted(right, Z, 1)
        blocks.append(right)
        if len(blocks) < lax.axis_size(Z):
            left = shifted(left, Z, -1)
            blocks.append(left)
    return blocks


def shards(
    tokens,
    norm_attn,
    w_query,
    w_key,
    w_value,
    w_out,
    head_bias,
    key_cache,
    value_cache,
    lengths,
    norm_ffn,
    w_group,
    w_fine,
    routes,
    e_gate,
    e_up,
    e_down,
    d_gate,
    d_up,
    d_down,
    w_mix,
):
    seq_count = tokens.shape[0]
    width_part = d_gate.shape[0]
    kv_local = key_cache.shape[1]
    head_dim = key_cache.shape[3]
    ep_size = lax.axis_size(EP)
    tps = lax.axis_size(TP)
    per_group = ep_size // GROUPS
    capacity = 2
    blocks = dense_weights(d_gate, d_up, d_down)

    h_first = normed(tokens, norm_attn).astype(jnp.bfloat16)
    queries = jnp.dot(h_first, w_query, preferred_element_type=jnp.float32).astype(jnp.bfloat16)
    new_keys = jnp.dot(h_first, w_key, preferred_element_type=jnp.float32).astype(jnp.bfloat16)
    new_values = jnp.dot(h_first, w_value, preferred_element_type=jnp.float32).astype(jnp.bfloat16)
    grouped = queries.reshape(seq_count, kv_local, -1, head_dim)
    heads_out = stick_read(
        grouped, key_cache, value_cache, lengths, head_bias.reshape(kv_local, -1)
    )
    partial_value = jnp.dot(heads_out, w_out, preferred_element_type=jnp.float32).astype(
        jnp.bfloat16
    )
    partial_value = lax.optimization_barrier(partial_value)
    attended = partial_value.astype(jnp.float32)
    for k in range(1, tps):
        attended = attended + shifted(partial_value, TP, k).astype(jnp.float32)
    resid = tokens.astype(jnp.float32) + attended
    h_second = normed(resid, norm_ffn).astype(jnp.bfloat16)
    column = lax.axis_index("tp") * width_part
    h_slice = lax.dynamic_slice_in_dim(h_second, column, width_part, 1)
    resid_slice = lax.dynamic_slice_in_dim(resid, column, width_part, 1)

    flat_routes = routes.T.reshape(-1)
    slot_ids = flat_routes * capacity + slot_ranks(flat_routes)
    onehot = (lax.iota(jnp.int32, ep_size * capacity)[:, None] == slot_ids[None, :]).astype(
        jnp.bfloat16
    )
    repeated = jnp.concatenate([h_slice] * TOP_K, axis=0)
    outbound = jnp.dot(onehot, repeated, preferred_element_type=jnp.float32)
    outbound = outbound.astype(jnp.bfloat16).reshape(ep_size, capacity, width_part)
    received = lax.all_to_all(outbound, EP, split_axis=0, concat_axis=0, tiled=True)

    here = jnp.concatenate(
        [h_second] + [shifted(h_second, Y, k) for k in range(1, lax.axis_size(Y))], axis=0
    )
    there = shifted(here, CORE, 1)
    parts = dense_parts(here, there, blocks, seq_count, width_part)
    dense_all = lax.all_to_all(parts, (Y, CORE, TP), split_axis=0, concat_axis=0, tiled=True)
    dense_slice = jnp.sum(dense_all.astype(jnp.float32), axis=0)

    flat_rows = received.reshape(-1, width_part)
    pre = expert_in(flat_rows, e_gate[0], e_up[0])
    act = pre[0].astype(jnp.float32)
    for k in range(1, tps):
        act = act + shifted(pre[k], TP, k).astype(jnp.float32)
    units = act.shape[1] // 2
    hidden = (silu(act[:, :units]) * act[:, units:]).astype(jnp.bfloat16)
    hidden = lax.optimization_barrier(hidden)
    hiddens = [hidden] + [shifted(hidden, TP, k) for k in range(1, tps)]
    result = expert_out(hiddens, e_down[0])
    returned = lax.all_to_all(
        result.reshape(received.shape), EP, split_axis=0, concat_axis=0, tiled=True
    )

    group_logits = jnp.dot(h_second, w_group, preferred_element_type=jnp.float32)
    fine_logits = jnp.dot(h_second, w_fine, preferred_element_type=jnp.float32)
    shares = route_weights(group_logits, fine_logits, routes, per_group)
    mix_gate = jax.nn.sigmoid(
        jnp.dot(h_second.astype(jnp.float32), w_mix, precision=lax.Precision.HIGHEST)
    )
    back = jnp.dot(
        onehot.T, returned.reshape(-1, width_part), preferred_element_type=jnp.float32
    ).reshape(TOP_K, seq_count, width_part)
    moe_slice = jnp.sum(back * shares.T[:, :, None], axis=0)
    mixed = resid_slice + moe_slice + mix_gate[:, None] * dense_slice
    return (
        mixed.astype(jnp.bfloat16),
        new_keys.reshape(seq_count, kv_local, head_dim),
        new_values.reshape(seq_count, kv_local, head_dim),
    )


def solution(mesh):
    torus = Mesh(mesh.devices.reshape(8, 4, 2, mesh.shape["tp"]), ("ep_0", "ep_1", "ep_2", "tp"))
    placed = (
        P(EP, None),
        P(),
        P(None, "tp"),
        P(None, "tp"),
        P(None, "tp"),
        P("tp", None),
        P("tp"),
        P(EP, "tp", None, None),
        P(EP, "tp", None, None),
        P(EP),
        P(),
        P(),
        P(),
        P(EP, None),
        P(EP, "tp", None),
        P(EP, "tp", None),
        P(EP, None, "tp"),
        P("tp", EP),
        P("tp", EP),
        P(EP, "tp"),
        P(),
    )
    return jax.shard_map(
        shards,
        mesh=torus,
        in_specs=placed,
        out_specs=(P(EP, "tp"), P(EP, "tp", None), P(EP, "tp", None)),
        check_vma=False,
    )
```

```python
import jax
import jax.numpy as jnp
from jax import lax
from jax.experimental import pallas as pl
from jax.experimental.pallas import tpu as pltpu
from jax.sharding import Mesh
from jax.sharding import PartitionSpec as P


EP = ("ep_0", "ep_1", "ep_2")
Z, Y, CORE, TP = "ep_0", "ep_1", "ep_2", "tp"

norm_eps = 1e-06
PIECE = 128
CHUNK = 8
EXTRA = 128
SLOTS = 16
VMEM_LIMIT = 12 * 2**20
NT = (((1,), (1,)), ((), ()))
F32 = jnp.float32
BF16 = jnp.bfloat16


def shifted(x, axis, step):
    size = lax.axis_size(axis)
    return lax.ppermute(x, axis, [(i, (i + step) % size) for i in range(size)])


def all_shifts(x, axis):
    return [x] + [shifted(x, axis, k) for k in range(1, lax.axis_size(axis))]


def silu(v):
    return v / (1.0 + jnp.exp(-v))


def dot(a, b):
    return jnp.dot(a, b, preferred_element_type=F32)


def dot_nt(a, b):
    return lax.dot_general(a, b, NT, preferred_element_type=F32)


def behind(axis, k):
    size = lax.axis_size(axis)
    return lax.rem(lax.axis_index(axis) - k + size, size)


def span(index, size):
    return pl.ds(pl.multiple_of(index * size, size), size)


def call(kernel, out, flops, moved, *operands, near=True, **more):
    if near:
        more["compiler_params"] = pltpu.CompilerParams(vmem_limit_bytes=VMEM_LIMIT)
    return pl.pallas_call(
        kernel,
        out_shape=out,
        cost_estimate=pl.CostEstimate(flops=flops, bytes_accessed=moved, transcendentals=0),
        **more,
    )(*operands)


def attention_kernel(
    lengths_ref, tokens_ref, gain_ref, bias_ref, wk_ref, wv_ref,
    wq_hbm, keys_hbm, values_hbm, wo_hbm,
    partial_ref, new_keys_ref, new_values_ref,
    wq_ref, keys_ref, values_ref, wo_ref,
    q_ref, split_ref, reach_ref, stop_ref, mixed_ref, heads_ref, sems,
):
    seq, heads, dim = q_ref.shape
    length = keys_ref.shape[2]
    pieces = length // PIECE
    chunks = seq // CHUNK

    def fetch(source, target, number):
        return pltpu.make_async_copy(source, target, sems.at[number])

    query_copy = fetch(wq_hbm, wq_ref, 0)
    key_copies = [
        fetch(keys_hbm.at[pl.ds(c * CHUNK, CHUNK)], keys_ref.at[pl.ds(c * CHUNK, CHUNK)], 2 + c)
        for c in range(chunks)
    ]
    value_copies = [
        fetch(
            values_hbm.at[pl.ds(c * CHUNK, CHUNK)],
            values_ref.at[pl.ds(c * CHUNK, CHUNK)],
            2 + chunks + c,
        )
        for c in range(chunks)
    ]
    out_copy = fetch(wo_hbm, wo_ref, 1)
    query_copy.start()
    for c in range(chunks):
        key_copies[c].start()
        value_copies[c].start()
    out_copy.start()

    wide = tokens_ref[...].astype(jnp.float32)
    scale = lax.rsqrt(jnp.mean(wide * wide, axis=-1, keepdims=True) + norm_eps)
    h_first = (wide * scale * gain_ref[...]).astype(jnp.bfloat16)
    for weight, target in ((wk_ref, new_keys_ref), (wv_ref, new_values_ref)):
        target[...] = lax.dot_general(
            h_first, weight[...], NT, preferred_element_type=jnp.float32
        ).astype(jnp.bfloat16)
    query_copy.wait()
    queries = jnp.dot(h_first, wq_ref[...], preferred_element_type=jnp.float32)
    for g in range(heads):
        q_ref[:, g, :] = queries[:, g * dim : (g + 1) * dim]

    row = lax.broadcasted_iota(jnp.int32, (2 * PIECE, 2 * PIECE), 0) % PIECE
    column = lax.broadcasted_iota(jnp.int32, (2 * PIECE, 2 * PIECE), 1)
    later = ((row > column) | (column >= PIECE)).astype(jnp.bfloat16)
    position = lax.broadcasted_iota(jnp.int32, (heads, PIECE), 1)
    head = lax.broadcasted_iota(jnp.int32, (heads, PIECE), 0)
    bias = jnp.full((heads, PIECE), bias_ref[0], jnp.float32)
    for g in range(1, heads):
        bias = jnp.where(head == g, bias_ref[g], bias)

    for c in range(chunks):
        key_copies[c].wait()
        for i in range(CHUNK):
            b = c * CHUNK + i
            scores = jnp.dot(
                q_ref[b].astype(jnp.bfloat16), keys_ref[b], preferred_element_type=jnp.float32
            )
            for p in range(pieces):
                s = scores[:, p * PIECE : (p + 1) * PIECE] * dim ** (-0.5) + bias
                inside = position < lengths_ref[b] - p * PIECE
                rest = jnp.log(1.0 + jnp.exp(-jnp.abs(s)))
                fail = jnp.where(inside, -(jnp.maximum(s, 0.0) + rest), 0.0)
                stop_ref[i, p] = jnp.where(inside, jnp.minimum(s, 0.0) - rest, -jnp.inf)
                high = fail.astype(jnp.bfloat16)
                low = (fail - high.astype(jnp.float32)).astype(jnp.bfloat16)
                at = (i * pieces + p) * heads
                split_ref[at : at + heads, :PIECE] = high.astype(jnp.float32)
                split_ref[at : at + heads, PIECE:] = low.astype(jnp.float32)
        reach_ref[...] = jnp.dot(
            split_ref[...].astype(jnp.bfloat16), later, preferred_element_type=jnp.float32
        )
        value_copies[c].wait()
        for i in range(CHUNK):
            b = c * CHUNK + i
            carried = None
            weights = [None] * pieces
            for p in reversed(range(pieces)):
                at = (i * pieces + p) * heads
                within = reach_ref[at : at + heads, :PIECE]
                whole = reach_ref[at : at + heads, PIECE:]
                exponent = stop_ref[i, p] + within
                if carried is not None:
                    exponent = exponent + carried
                weights[p] = jnp.exp(exponent)
                carried = whole if carried is None else carried + whole
            stick = jnp.concatenate(weights, axis=1).astype(jnp.bfloat16)
            mixed_ref[b] = lax.dot_general(
                stick, values_ref[b], NT, preferred_element_type=jnp.float32
            )
    for g in range(heads):
        heads_ref[:, g * dim : (g + 1) * dim] = mixed_ref[:, g, :]
    out_copy.wait()
    partial_ref[...] = jnp.dot(
        heads_ref[...].astype(jnp.bfloat16), wo_ref[...], preferred_element_type=jnp.float32
    ).astype(jnp.bfloat16)


def attention(tokens, gain, wq, wk, wv, wo, bias, keys, values, lengths):
    seq, width = tokens.shape
    dim, length = keys.shape[2], keys.shape[3]
    heads = bias.shape[0]
    keys, values = keys[:, 0], values[:, 0]
    pieces = length // PIECE
    rows = CHUNK * pieces * heads
    vmem = pl.BlockSpec(memory_space=pltpu.VMEM)
    anywhere = pl.BlockSpec(memory_space=pltpu.HBM)
    smem = pl.BlockSpec(memory_space=pltpu.SMEM)
    return pl.pallas_call(
        attention_kernel,
        out_shape=(
            jax.ShapeDtypeStruct((seq, width), jnp.bfloat16),
            jax.ShapeDtypeStruct((seq, dim), jnp.bfloat16),
            jax.ShapeDtypeStruct((seq, dim), jnp.bfloat16),
        ),
        in_specs=[smem, vmem, vmem, smem, vmem, vmem] + [anywhere] * 4,
        out_specs=(vmem, vmem, vmem),
        scratch_shapes=[
            pltpu.VMEM(wq.shape, jnp.bfloat16),
            pltpu.VMEM(keys.shape, jnp.bfloat16),
            pltpu.VMEM(values.shape, jnp.bfloat16),
            pltpu.VMEM(wo.shape, jnp.bfloat16),
            pltpu.VMEM((seq, heads, dim), jnp.float32),
            pltpu.VMEM((rows, 2 * PIECE), jnp.float32),
            pltpu.VMEM((rows, 2 * PIECE), jnp.float32),
            pltpu.VMEM((CHUNK, pieces, heads, PIECE), jnp.float32),
            pltpu.VMEM((seq, heads, dim), jnp.float32),
            pltpu.VMEM((seq, heads * dim), jnp.float32),
            pltpu.SemaphoreType.DMA((2 + 2 * (seq // CHUNK),)),
        ],
        cost_estimate=pl.CostEstimate(
            flops=400_000_000, bytes_accessed=11_000_000, transcendentals=600_000
        ),
        name="attention",
    )(lengths, tokens, gain[None, :], bias, wk, wv, wq, keys, values, wo)


def prepare_kernel(gate_ref, up_ref, *outs_and_scratch):
    outs, (gates, ups) = outs_and_scratch[:-2], outs_and_scratch[-2:]
    units = outs[0].shape[0] // 2
    gates[...] = gate_ref[...].T
    ups[...] = up_ref[...].T
    for k, out in enumerate(outs):
        at = span(behind(TP, -k), units)
        out[:units, :] = gates[at, :]
        out[units:, :] = ups[at, :]


def prepare(d_gate, d_up):
    tps = lax.axis_size(TP)
    width, units = d_gate.shape
    one = jax.ShapeDtypeStruct((2 * units // tps, width), BF16)
    turned = pltpu.VMEM((units, width), BF16)
    return call(
        prepare_kernel, (one,) * tps, 0, 600_000, d_gate, d_up,
        scratch_shapes=[turned, turned],
    )


def norm_kernel(tokens_ref, gain_ref, routes_ref, *refs):
    parts, (payload_ref, slice_ref, resid_ref) = refs[:-3], refs[-3:]
    seq, width = tokens_ref.shape
    attended = parts[0][...].astype(F32)
    for part in parts[1:]:
        attended = attended + part[...].astype(F32)
    resid = tokens_ref[...].astype(F32) + attended
    resid_ref[...] = resid
    scale = lax.rsqrt(jnp.mean(resid * resid, axis=-1, keepdims=True) + norm_eps)
    payload_ref[:, :width] = (resid * scale * gain_ref[...]).astype(BF16)
    lane = lax.broadcasted_iota(jnp.int32, (seq, EXTRA), 1)
    routes = routes_ref[...]
    named = jnp.where(lane == 0, routes[:, 0:1], jnp.where(lane == 1, routes[:, 1:2], 0))
    payload_ref[:, width:] = named.astype(F32).astype(BF16)
    slice_ref[...] = resid_ref[:, span(lax.axis_index(TP), slice_ref.shape[1])]


def norm_payload(tokens, gain, routes, parts):
    seq, width = tokens.shape
    return call(
        norm_kernel,
        (
            jax.ShapeDtypeStruct((seq, width + EXTRA), BF16),
            jax.ShapeDtypeStruct((seq, width // lax.axis_size(TP)), F32),
        ),
        1_000_000, 600_000, tokens, gain[None, :], routes, *parts,
        scratch_shapes=[pltpu.VMEM((seq, width), F32)],
    )


def group_routes(tokens):
    width = tokens[0].shape[1] - EXTRA
    extra = jnp.concatenate([ref[:, width:].astype(F32) for ref in tokens], axis=0)
    first, second = extra[:, 0:1], extra[:, 1:2]
    slots = lax.axis_size(Z) * SLOTS
    lane = lax.broadcasted_iota(jnp.int32, (extra.shape[0], slots), 1)
    plane = lax.axis_size(Y) * lax.axis_size(CORE)
    place = lax.axis_index(Y) * lax.axis_size(CORE) + lax.axis_index(CORE)
    expert = ((lane // SLOTS) * plane + place).astype(F32)
    return first, second, expert, (lane % SLOTS).astype(F32)


def select_kernel(*refs):
    tokens, (rows_ref, hot_ref) = refs[:-2], refs[-2:]
    part = rows_ref.shape[1]
    first, second, expert, slot = group_routes(tokens)
    match = ((first == expert) | (second == expert)).astype(F32)
    count = match.shape[0]
    row = lax.broadcasted_iota(jnp.int32, (count, count), 0)
    column = lax.broadcasted_iota(jnp.int32, (count, count), 1)
    rank = dot((column < row).astype(BF16), match.astype(BF16))
    hot = jnp.where(rank == slot, match, 0.0)
    hot_ref[...] = hot.astype(BF16)
    mine = jnp.concatenate(
        [ref[:, span(lax.axis_index(TP), part)].astype(F32) for ref in tokens], axis=0
    ).astype(BF16)
    rows_ref[...] = dot(hot.T.astype(BF16), mine).astype(BF16)


def select(tokens, part):
    slots = lax.axis_size(Z) * SLOTS
    count = len(tokens) * tokens[0].shape[0]
    return call(
        select_kernel,
        (
            jax.ShapeDtypeStruct((slots, part), BF16),
            jax.ShapeDtypeStruct((count, slots), BF16),
        ),
        40_000_000, 1_000_000, *tokens,
    )


def share_kernel(hot_ref, group_ref, fine_ref, mix_ref, *refs):
    tokens, (high_ref, low_ref, gate_ref) = refs[:-3], refs[-3:]
    width = group_ref.shape[1]
    per_group = fine_ref.shape[0] // group_ref.shape[0]
    rows = jnp.concatenate([ref[:, :width].astype(F32) for ref in tokens], axis=0)
    narrow = rows.astype(BF16)
    group_logits = dot_nt(narrow, group_ref[...])
    fine_logits = dot_nt(narrow, fine_ref[...])
    first, second, expert, _ = group_routes(tokens)
    group = lax.broadcasted_iota(jnp.int32, group_logits.shape, 1)
    own = (first.astype(jnp.int32) // per_group) == group
    own_logit = jnp.sum(jnp.where(own, group_logits, 0.0), axis=1, keepdims=True)
    group_share = 1.0 / jnp.sum(jnp.exp(group_logits - own_logit), axis=1, keepdims=True)
    fine = lax.broadcasted_iota(jnp.int32, fine_logits.shape, 1).astype(F32)
    picked = [
        jnp.sum(jnp.where(fine == chosen, fine_logits, 0.0), axis=1, keepdims=True)
        for chosen in (first, second)
    ]
    weight = 0.0
    for chosen, here, there in ((first, 0, 1), (second, 1, 0)):
        share = group_share * (1.0 / (1.0 + jnp.exp(picked[there] - picked[here])))
        weight = weight + jnp.where(chosen == expert, share, 0.0)
    weight = weight * hot_ref[...].astype(F32)
    high = weight.astype(BF16)
    high_ref[...] = high
    low_ref[...] = (weight - high.astype(F32)).astype(BF16)
    mix = jnp.sum(rows * mix_ref[...], axis=1, keepdims=True)
    gate_ref[...] = jnp.broadcast_to(1.0 / (1.0 + jnp.exp(-mix)), gate_ref.shape)


def share_weights(hot, w_group, w_fine, w_mix, tokens):
    table = jax.ShapeDtypeStruct(hot.shape, BF16)
    return call(
        share_kernel,
        (table, table, jax.ShapeDtypeStruct((hot.shape[0], EXTRA), F32)),
        60_000_000, 1_500_000, hot, w_group.T, w_fine.T, w_mix[None, :], *tokens, near=False,
    )


def expert_in_kernel(rows_ref, gate_ref, up_ref, out_ref):
    units = gate_ref.shape[1]
    rows = rows_ref[...]
    out_ref[:, :units] = dot(rows, gate_ref[...]).astype(BF16)
    out_ref[:, units:] = dot(rows, up_ref[...]).astype(BF16)


def expert_in(rows, gate, up):
    return call(
        expert_in_kernel,
        jax.ShapeDtypeStruct((rows.shape[0], 2 * gate.shape[1]), BF16),
        140_000_000, 1_400_000, rows, gate, up,
    )


def expert_out_kernel(*refs):
    parts, (down_ref, out_ref) = refs[:-2], refs[-2:]
    units = down_ref.shape[0]
    act = parts[0][...].astype(F32)
    for part in parts[1:]:
        act = act + part[...].astype(F32)
    hidden = (silu(act[:, :units]) * act[:, units:]).astype(BF16)
    out_ref[...] = dot(hidden, down_ref[...]).astype(BF16)


def expert_out(parts, down):
    return call(
        expert_out_kernel,
        jax.ShapeDtypeStruct((parts[0].shape[0], down.shape[1]), BF16),
        70_000_000, 1_800_000, *parts, down,
    )


def dense_in_kernel(*refs):
    out_ref = refs[-1]
    planes, tps = lax.axis_size(Z), lax.axis_size(TP)
    tokens, blocks = refs[: -planes - 1], refs[-planes - 1 : -1]
    width = blocks[0].shape[1]
    units = out_ref.shape[1] // planes
    gate = up = 0.0
    for k in range(tps):
        at = span(behind(TP, k), width)
        rows = jnp.concatenate([ref[:, at].astype(F32) for ref in tokens], axis=0).astype(BF16)
        low, mid, top = 2 * k * units, (2 * k + 1) * units, (2 * k + 2) * units
        gate = gate + dot_nt(rows, jnp.concatenate([b[low:mid, :] for b in blocks], axis=0))
        up = up + dot_nt(rows, jnp.concatenate([b[mid:top, :] for b in blocks], axis=0))
    out_ref[...] = (silu(gate) * up).astype(BF16)


def dense_in(tokens, blocks):
    count = len(tokens) * tokens[0].shape[0]
    rows, width = blocks[0].shape
    whole = pl.BlockSpec(memory_space=pltpu.VMEM)
    upper = pl.BlockSpec((rows * 2 // 3, width), lambda i: (0, 0))
    kept = lambda shape: pl.BlockSpec(shape, lambda i: (0, 0))
    return call(
        dense_in_kernel,
        jax.ShapeDtypeStruct((count, rows * 2 // 3), BF16),
        400_000_000, 3_000_000, *tokens, *blocks, near=False,
        grid=(1,),
        in_specs=[kept(x.shape) for x in tokens] + [upper] * len(blocks),
        out_specs=kept((count, rows * 2 // 3)),
    )


def dense_out_kernel(*refs):
    gate_ref, out_ref = refs[-2:]
    planes, tps = lax.axis_size(Z), lax.axis_size(TP)
    hiddens, blocks = refs[:tps], refs[tps : tps + planes]
    units = blocks[0].shape[0] // tps
    total = 0.0
    for k in range(tps):
        at = span(behind(TP, k), units)
        total = total + dot(
            hiddens[k][...], jnp.concatenate([b[at, :] for b in blocks], axis=0)
        )
    out_ref[...] = total * gate_ref[:, 0:1]


def dense_out(hiddens, blocks, gate):
    count = hiddens[0].shape[0]
    rows, width = blocks[0].shape
    kept = lambda shape: pl.BlockSpec(shape, lambda i: (0, 0))
    lower = pl.BlockSpec((rows // 3, width), lambda i: (2, 0))
    return call(
        dense_out_kernel,
        jax.ShapeDtypeStruct((count, width), F32),
        400_000_000, 2_000_000, *hiddens, *blocks, gate, near=False,
        grid=(1,),
        in_specs=[kept(x.shape) for x in hiddens] + [lower] * len(blocks) + [kept(gate.shape)],
        out_specs=kept((count, width)),
    )


def gather_kernel(dense_ref, rows_ref, high_ref, low_ref, out_ref):
    rows = rows_ref[...]
    total = dense_ref[...] + (dot(high_ref[...], rows) + dot(low_ref[...], rows))
    seq = out_ref.shape[1]
    ys, c = lax.axis_size(Y), lax.axis_index(CORE)
    for other in range(2):
        core = c if other == 0 else 1 - c
        for j in range(ys):
            at = (other * ys + j) * seq
            out_ref[behind(Y, j) * 2 + core] = total[at : at + seq].astype(BF16)


def gather_rows(dense, rows, high, low, seq):
    return call(
        gather_kernel,
        jax.ShapeDtypeStruct((dense.shape[0] // seq, seq, dense.shape[1]), BF16),
        60_000_000, 1_000_000, dense, rows, high, low, near=False,
    )


def finish_kernel(resid_ref, parts_ref, out_ref):
    total = resid_ref[...]
    for i in range(parts_ref.shape[0]):
        total = total + parts_ref[i].astype(F32)
    out_ref[...] = total.astype(BF16)


def finish(resid, parts):
    return call(finish_kernel, jax.ShapeDtypeStruct(resid.shape, BF16), 0, 400_000, resid, parts)


def along_z(own):
    blocks = [own]
    right = left = own
    for _ in range(1, lax.axis_size(Z) // 2 + 1):
        right = shifted(right, Z, 1)
        blocks.append(right)
        if len(blocks) < lax.axis_size(Z):
            left = shifted(left, Z, -1)
            blocks.append(left)
    return blocks


def over_z(rows):
    planes = lax.axis_size(Z)
    shaped = rows.reshape(planes, -1, rows.shape[1])
    return lax.all_to_all(shaped, Z, split_axis=0, concat_axis=0, tiled=True).reshape(rows.shape)


def shards(
    tokens,
    norm_attn,
    w_query,
    w_key,
    w_value,
    w_out,
    head_bias,
    key_cache,
    value_cache,
    lengths,
    norm_ffn,
    w_group,
    w_fine,
    routes,
    e_gate,
    e_up,
    e_down,
    d_gate,
    d_up,
    d_down,
    w_mix,
):
    seq_count = tokens.shape[0]
    width_part = d_gate.shape[0]
    kv_local = key_cache.shape[1]
    head_dim = key_cache.shape[3]
    wide = prepare(d_gate, d_up)
    arrived = [wide[0]] + [shifted(wide[k], TP, k) for k in range(1, len(wide))]
    partial_value, new_keys, new_values = attention(
        tokens,
        norm_attn,
        w_query,
        w_key.T,
        w_value.T,
        w_out,
        head_bias,
        key_cache.transpose(0, 1, 3, 2),
        value_cache.transpose(0, 1, 3, 2),
        lengths,
    )
    parts = all_shifts(partial_value, TP)
    own = jnp.concatenate([*arrived, d_down], axis=0)
    blocks = along_z(own)
    payload, resid = norm_payload(tokens, norm_ffn, routes, parts)
    here = all_shifts(payload, Y)
    group = here + [shifted(x, CORE, 1) for x in here]
    rows, hot = select(group, width_part)
    rows = over_z(rows)
    pre = expert_in(rows, e_gate[0], e_up[0])
    pres = all_shifts(pre, TP)
    result = expert_out(pres, e_down[0])
    returned = over_z(result)
    high, low, gate = share_weights(hot, w_group, w_fine, w_mix, group)
    hidden = dense_in(group, blocks)
    hiddens = all_shifts(hidden, TP)
    dense = dense_out(hiddens, blocks, gate)
    parts = gather_rows(dense, returned, high, low, seq_count)
    parts = lax.all_to_all(parts, (Y, CORE), split_axis=0, concat_axis=0, tiled=True)
    mixed = finish(resid, parts)
    return (
        mixed,
        new_keys.reshape(seq_count, kv_local, head_dim),
        new_values.reshape(seq_count, kv_local, head_dim),
    )


def solution(mesh):
    torus = Mesh(mesh.devices.reshape(8, 4, 2, mesh.shape["tp"]), ("ep_0", "ep_1", "ep_2", "tp"))
    placed = (
        P(EP, None),
        P(),
        P(None, "tp"),
        P(None, "tp"),
        P(None, "tp"),
        P("tp", None),
        P("tp"),
        P(EP, "tp", None, None),
        P(EP, "tp", None, None),
        P(EP),
        P(),
        P(),
        P(),
        P(EP, None),
        P(EP, "tp", None),
        P(EP, "tp", None),
        P(EP, None, "tp"),
        P("tp", EP),
        P("tp", EP),
        P(EP, "tp"),
        P(),
    )
    return jax.shard_map(
        shards,
        mesh=torus,
        in_specs=placed,
        out_specs=(P(EP, "tp"), P(EP, "tp", None), P(EP, "tp", None)),
        check_vma=False,
    )
```

```python
import jax
import jax.numpy as jnp
from jax import lax
from jax.experimental import pallas as pl
from jax.experimental.pallas import tpu as pltpu
from jax.sharding import Mesh
from jax.sharding import PartitionSpec as P


EP = ("ep_0", "ep_1", "ep_2")
Z, Y, CORE, TP = "ep_0", "ep_1", "ep_2", "tp"

norm_eps = 1e-06
PIECE = 128
CHUNK = 8
EXTRA = 128
SLOTS = 16
VMEM_LIMIT = 12 * 2**20
NT = (((1,), (1,)), ((), ()))
F32 = jnp.float32
BF16 = jnp.bfloat16


def shifted(x, axis, step):
    size = lax.axis_size(axis)
    return lax.ppermute(x, axis, [(i, (i + step) % size) for i in range(size)])


def all_shifts(x, axis):
    return [x] + [shifted(x, axis, k) for k in range(1, lax.axis_size(axis))]


def silu(v):
    return v / (1.0 + jnp.exp(-v))


def dot(a, b):
    return jnp.dot(a, b, preferred_element_type=F32)


def dot_nt(a, b):
    return lax.dot_general(a, b, NT, preferred_element_type=F32)


def behind(axis, k):
    size = lax.axis_size(axis)
    return lax.rem(lax.axis_index(axis) - k + size, size)


def span(index, size):
    return pl.ds(pl.multiple_of(index * size, size), size)


def call(kernel, out, flops, moved, *operands, near=True, **more):
    if near:
        more["compiler_params"] = pltpu.CompilerParams(vmem_limit_bytes=VMEM_LIMIT)
    return pl.pallas_call(
        kernel,
        out_shape=out,
        cost_estimate=pl.CostEstimate(flops=flops, bytes_accessed=moved, transcendentals=0),
        **more,
    )(*operands)


def attention_kernel(
    lengths_ref, tokens_ref, gain_ref, bias_ref, wk_ref, wv_ref,
    wq_hbm, keys_hbm, values_hbm, wo_hbm,
    partial_ref, new_keys_ref, new_values_ref,
    wq_ref, keys_ref, values_ref, wo_ref,
    q_ref, split_ref, reach_ref, stop_ref, mixed_ref, heads_ref, sems,
):
    seq, heads, dim = q_ref.shape
    length = keys_ref.shape[2]
    pieces = length // PIECE
    chunks = seq // CHUNK

    def fetch(source, target, number):
        return pltpu.make_async_copy(source, target, sems.at[number])

    query_copy = fetch(wq_hbm, wq_ref, 0)
    key_copies = [
        fetch(keys_hbm.at[pl.ds(c * CHUNK, CHUNK)], keys_ref.at[pl.ds(c * CHUNK, CHUNK)], 2 + c)
        for c in range(chunks)
    ]
    value_copies = [
        fetch(
            values_hbm.at[pl.ds(c * CHUNK, CHUNK)],
            values_ref.at[pl.ds(c * CHUNK, CHUNK)],
            2 + chunks + c,
        )
        for c in range(chunks)
    ]
    out_copy = fetch(wo_hbm, wo_ref, 1)
    query_copy.start()
    for c in range(chunks):
        key_copies[c].start()
        value_copies[c].start()
    out_copy.start()

    wide = tokens_ref[...].astype(jnp.float32)
    scale = lax.rsqrt(jnp.mean(wide * wide, axis=-1, keepdims=True) + norm_eps)
    h_first = (wide * scale * gain_ref[...]).astype(jnp.bfloat16)
    for weight, target in ((wk_ref, new_keys_ref), (wv_ref, new_values_ref)):
        target[...] = lax.dot_general(
            h_first, weight[...], NT, preferred_element_type=jnp.float32
        ).astype(jnp.bfloat16)
    query_copy.wait()
    queries = jnp.dot(h_first, wq_ref[...], preferred_element_type=jnp.float32)
    for g in range(heads):
        q_ref[:, g, :] = queries[:, g * dim : (g + 1) * dim]

    row = lax.broadcasted_iota(jnp.int32, (2 * PIECE, 2 * PIECE), 0) % PIECE
    column = lax.broadcasted_iota(jnp.int32, (2 * PIECE, 2 * PIECE), 1)
    later = ((row > column) | (column >= PIECE)).astype(jnp.bfloat16)
    position = lax.broadcasted_iota(jnp.int32, (heads, PIECE), 1)
    head = lax.broadcasted_iota(jnp.int32, (heads, PIECE), 0)
    bias = jnp.full((heads, PIECE), bias_ref[0], jnp.float32)
    for g in range(1, heads):
        bias = jnp.where(head == g, bias_ref[g], bias)

    for c in range(chunks):
        key_copies[c].wait()
        for i in range(CHUNK):
            b = c * CHUNK + i
            scores = jnp.dot(
                q_ref[b].astype(jnp.bfloat16), keys_ref[b], preferred_element_type=jnp.float32
            )
            for p in range(pieces):
                s = scores[:, p * PIECE : (p + 1) * PIECE] * dim ** (-0.5) + bias
                inside = position < lengths_ref[b] - p * PIECE
                rest = jnp.log(1.0 + jnp.exp(-jnp.abs(s)))
                fail = jnp.where(inside, -(jnp.maximum(s, 0.0) + rest), 0.0)
                stop_ref[i, p] = jnp.where(inside, jnp.minimum(s, 0.0) - rest, -jnp.inf)
                high = fail.astype(jnp.bfloat16)
                low = (fail - high.astype(jnp.float32)).astype(jnp.bfloat16)
                at = (i * pieces + p) * heads
                split_ref[at : at + heads, :PIECE] = high.astype(jnp.float32)
                split_ref[at : at + heads, PIECE:] = low.astype(jnp.float32)
        reach_ref[...] = jnp.dot(
            split_ref[...].astype(jnp.bfloat16), later, preferred_element_type=jnp.float32
        )
        value_copies[c].wait()
        for i in range(CHUNK):
            b = c * CHUNK + i
            carried = None
            weights = [None] * pieces
            for p in reversed(range(pieces)):
                at = (i * pieces + p) * heads
                within = reach_ref[at : at + heads, :PIECE]
                whole = reach_ref[at : at + heads, PIECE:]
                exponent = stop_ref[i, p] + within
                if carried is not None:
                    exponent = exponent + carried
                weights[p] = jnp.exp(exponent)
                carried = whole if carried is None else carried + whole
            stick = jnp.concatenate(weights, axis=1).astype(jnp.bfloat16)
            mixed_ref[b] = lax.dot_general(
                stick, values_ref[b], NT, preferred_element_type=jnp.float32
            )
    for g in range(heads):
        heads_ref[:, g * dim : (g + 1) * dim] = mixed_ref[:, g, :]
    out_copy.wait()
    partial_ref[...] = jnp.dot(
        heads_ref[...].astype(jnp.bfloat16), wo_ref[...], preferred_element_type=jnp.float32
    ).astype(jnp.bfloat16)


def attention(tokens, gain, wq, wk, wv, wo, bias, keys, values, lengths):
    seq, width = tokens.shape
    dim, length = keys.shape[2], keys.shape[3]
    heads = bias.shape[0]
    keys, values = keys[:, 0], values[:, 0]
    pieces = length // PIECE
    rows = CHUNK * pieces * heads
    vmem = pl.BlockSpec(memory_space=pltpu.VMEM)
    anywhere = pl.BlockSpec(memory_space=pltpu.HBM)
    smem = pl.BlockSpec(memory_space=pltpu.SMEM)
    return pl.pallas_call(
        attention_kernel,
        out_shape=(
            jax.ShapeDtypeStruct((seq, width), jnp.bfloat16),
            jax.ShapeDtypeStruct((seq, dim), jnp.bfloat16),
            jax.ShapeDtypeStruct((seq, dim), jnp.bfloat16),
        ),
        in_specs=[smem, vmem, vmem, smem, vmem, vmem] + [anywhere] * 4,
        out_specs=(vmem, vmem, vmem),
        scratch_shapes=[
            pltpu.VMEM(wq.shape, jnp.bfloat16),
            pltpu.VMEM(keys.shape, jnp.bfloat16),
            pltpu.VMEM(values.shape, jnp.bfloat16),
            pltpu.VMEM(wo.shape, jnp.bfloat16),
            pltpu.VMEM((seq, heads, dim), jnp.float32),
            pltpu.VMEM((rows, 2 * PIECE), jnp.float32),
            pltpu.VMEM((rows, 2 * PIECE), jnp.float32),
            pltpu.VMEM((CHUNK, pieces, heads, PIECE), jnp.float32),
            pltpu.VMEM((seq, heads, dim), jnp.float32),
            pltpu.VMEM((seq, heads * dim), jnp.float32),
            pltpu.SemaphoreType.DMA((2 + 2 * (seq // CHUNK),)),
        ],
        cost_estimate=pl.CostEstimate(
            flops=400_000_000, bytes_accessed=11_000_000, transcendentals=600_000
        ),
        name="attention",
    )(lengths, tokens, gain[None, :], bias, wk, wv, wq, keys, values, wo)


def prepare_kernel(gate_ref, up_ref, *outs_and_scratch):
    outs, (gates, ups) = outs_and_scratch[:-2], outs_and_scratch[-2:]
    units = outs[0].shape[0] // 2
    gates[...] = gate_ref[...].T
    ups[...] = up_ref[...].T
    for k, out in enumerate(outs):
        at = span(behind(TP, -k), units)
        out[:units, :] = gates[at, :]
        out[units:, :] = ups[at, :]


def prepare(d_gate, d_up):
    tps = lax.axis_size(TP)
    width, units = d_gate.shape
    one = jax.ShapeDtypeStruct((2 * units // tps, width), BF16)
    turned = pltpu.VMEM((units, width), BF16)
    return call(
        prepare_kernel, (one,) * tps, 0, 600_000, d_gate, d_up,
        scratch_shapes=[turned, turned],
    )


def norm_kernel(tokens_ref, gain_ref, routes_ref, *refs):
    parts, (payload_ref, slice_ref, resid_ref) = refs[:-3], refs[-3:]
    seq, width = tokens_ref.shape
    attended = parts[0][...].astype(F32)
    for part in parts[1:]:
        attended = attended + part[...].astype(F32)
    resid = tokens_ref[...].astype(F32) + attended
    resid_ref[...] = resid
    scale = lax.rsqrt(jnp.mean(resid * resid, axis=-1, keepdims=True) + norm_eps)
    payload_ref[:, :width] = (resid * scale * gain_ref[...]).astype(BF16)
    lane = lax.broadcasted_iota(jnp.int32, (seq, EXTRA), 1)
    routes = routes_ref[...]
    named = jnp.where(lane == 0, routes[:, 0:1], jnp.where(lane == 1, routes[:, 1:2], 0))
    payload_ref[:, width:] = named.astype(F32).astype(BF16)
    slice_ref[...] = resid_ref[:, span(lax.axis_index(TP), slice_ref.shape[1])]


def norm_payload(tokens, gain, routes, parts):
    seq, width = tokens.shape
    return call(
        norm_kernel,
        (
            jax.ShapeDtypeStruct((seq, width + EXTRA), BF16),
            jax.ShapeDtypeStruct((seq, width // lax.axis_size(TP)), F32),
        ),
        1_000_000, 600_000, tokens, gain[None, :], routes, *parts,
        scratch_shapes=[pltpu.VMEM((seq, width), F32)],
    )


def group_routes(tokens):
    width = tokens[0].shape[1] - EXTRA
    extra = jnp.concatenate([ref[:, width:].astype(F32) for ref in tokens], axis=0)
    first, second = extra[:, 0:1], extra[:, 1:2]
    slots = lax.axis_size(Z) * SLOTS
    lane = lax.broadcasted_iota(jnp.int32, (extra.shape[0], slots), 1)
    plane = lax.axis_size(Y) * lax.axis_size(CORE)
    place = lax.axis_index(Y) * lax.axis_size(CORE) + lax.axis_index(CORE)
    expert = ((lane // SLOTS) * plane + place).astype(F32)
    return first, second, expert, (lane % SLOTS).astype(F32)


def select_kernel(*refs):
    tokens, (rows_ref, hot_ref) = refs[:-2], refs[-2:]
    part = rows_ref.shape[1]
    first, second, expert, slot = group_routes(tokens)
    match = ((first == expert) | (second == expert)).astype(F32)
    count = match.shape[0]
    row = lax.broadcasted_iota(jnp.int32, (count, count), 0)
    column = lax.broadcasted_iota(jnp.int32, (count, count), 1)
    rank = dot((column < row).astype(BF16), match.astype(BF16))
    hot = jnp.where(rank == slot, match, 0.0)
    hot_ref[...] = hot.astype(BF16)
    mine = jnp.concatenate(
        [ref[:, span(lax.axis_index(TP), part)].astype(F32) for ref in tokens], axis=0
    ).astype(BF16)
    rows_ref[...] = dot(hot.T.astype(BF16), mine).astype(BF16)


def select(tokens, part):
    slots = lax.axis_size(Z) * SLOTS
    count = len(tokens) * tokens[0].shape[0]
    return call(
        select_kernel,
        (
            jax.ShapeDtypeStruct((slots, part), BF16),
            jax.ShapeDtypeStruct((count, slots), BF16),
        ),
        40_000_000, 1_000_000, *tokens,
    )


def share_kernel(hot_ref, group_ref, fine_ref, mix_ref, *refs):
    tokens, (high_ref, low_ref, gate_ref) = refs[:-3], refs[-3:]
    width = group_ref.shape[1]
    per_group = fine_ref.shape[0] // group_ref.shape[0]
    rows = jnp.concatenate([ref[:, :width].astype(F32) for ref in tokens], axis=0)
    narrow = rows.astype(BF16)
    group_logits = dot_nt(narrow, group_ref[...])
    fine_logits = dot_nt(narrow, fine_ref[...])
    first, second, expert, _ = group_routes(tokens)
    group = lax.broadcasted_iota(jnp.int32, group_logits.shape, 1)
    own = (first.astype(jnp.int32) // per_group) == group
    own_logit = jnp.sum(jnp.where(own, group_logits, 0.0), axis=1, keepdims=True)
    group_share = 1.0 / jnp.sum(jnp.exp(group_logits - own_logit), axis=1, keepdims=True)
    fine = lax.broadcasted_iota(jnp.int32, fine_logits.shape, 1).astype(F32)
    picked = [
        jnp.sum(jnp.where(fine == chosen, fine_logits, 0.0), axis=1, keepdims=True)
        for chosen in (first, second)
    ]
    weight = 0.0
    for chosen, here, there in ((first, 0, 1), (second, 1, 0)):
        share = group_share * (1.0 / (1.0 + jnp.exp(picked[there] - picked[here])))
        weight = weight + jnp.where(chosen == expert, share, 0.0)
    weight = weight * hot_ref[...].astype(F32)
    high = weight.astype(BF16)
    high_ref[...] = high
    low_ref[...] = (weight - high.astype(F32)).astype(BF16)
    mix = jnp.sum(rows * mix_ref[...], axis=1, keepdims=True)
    gate_ref[...] = jnp.broadcast_to(1.0 / (1.0 + jnp.exp(-mix)), gate_ref.shape)


def share_weights(hot, w_group, w_fine, w_mix, tokens):
    table = jax.ShapeDtypeStruct(hot.shape, BF16)
    return call(
        share_kernel,
        (table, table, jax.ShapeDtypeStruct((hot.shape[0], EXTRA), F32)),
        60_000_000, 1_500_000, hot, w_group.T, w_fine.T, w_mix[None, :], *tokens, near=False,
    )


def expert_in_kernel(rows_ref, gate_ref, up_ref, *outs):
    units = outs[0].shape[1] // 2
    rows = rows_ref[...]
    for k, out in enumerate(outs):
        at = span(behind(TP, -k), units)
        both = jnp.concatenate([gate_ref[:, at], up_ref[:, at]], axis=1)
        out[...] = dot(rows, both).astype(BF16)


def expert_in(rows, gate, up):
    tps = lax.axis_size(TP)
    one = jax.ShapeDtypeStruct((rows.shape[0], 2 * gate.shape[1] // tps), BF16)
    return call(expert_in_kernel, (one,) * tps, 140_000_000, 1_400_000, rows, gate, up)


def expert_act_kernel(*refs):
    parts, out_ref = refs[:-1], refs[-1]
    units = out_ref.shape[1]
    act = parts[0][...].astype(F32)
    for part in parts[1:]:
        act = act + part[...].astype(F32)
    out_ref[...] = (silu(act[:, :units]) * act[:, units:]).astype(BF16)


def expert_act(parts):
    rows, width = parts[0].shape
    return call(
        expert_act_kernel,
        jax.ShapeDtypeStruct((rows, width // 2), BF16),
        1_000_000, 300_000, *parts,
    )


def expert_out_kernel(*refs):
    hiddens, (down_ref, out_ref) = refs[:-2], refs[-2:]
    units = hiddens[0].shape[1]
    total = 0.0
    for k, hidden in enumerate(hiddens):
        total = total + dot(hidden[...], down_ref[span(behind(TP, k), units), :])
    out_ref[...] = total.astype(BF16)


def expert_out(hiddens, down):
    return call(
        expert_out_kernel,
        jax.ShapeDtypeStruct((hiddens[0].shape[0], down.shape[1]), BF16),
        70_000_000, 800_000, *hiddens, down,
    )


def dense_in_kernel(*refs):
    out_ref = refs[-1]
    planes, tps = lax.axis_size(Z), lax.axis_size(TP)
    tokens, blocks = refs[: -planes - 1], refs[-planes - 1 : -1]
    width = blocks[0].shape[1]
    units = out_ref.shape[1] // planes
    gate = up = 0.0
    for k in range(tps):
        at = span(behind(TP, k), width)
        rows = jnp.concatenate([ref[:, at].astype(F32) for ref in tokens], axis=0).astype(BF16)
        low, mid, top = 2 * k * units, (2 * k + 1) * units, (2 * k + 2) * units
        gate = gate + dot_nt(rows, jnp.concatenate([b[low:mid, :] for b in blocks], axis=0))
        up = up + dot_nt(rows, jnp.concatenate([b[mid:top, :] for b in blocks], axis=0))
    out_ref[...] = (silu(gate) * up).astype(BF16)


def dense_in(tokens, blocks):
    count = len(tokens) * tokens[0].shape[0]
    rows, width = blocks[0].shape
    whole = pl.BlockSpec(memory_space=pltpu.VMEM)
    upper = pl.BlockSpec((rows * 2 // 3, width), lambda i: (0, 0))
    kept = lambda shape: pl.BlockSpec(shape, lambda i: (0, 0))
    return call(
        dense_in_kernel,
        jax.ShapeDtypeStruct((count, rows * 2 // 3), BF16),
        400_000_000, 3_000_000, *tokens, *blocks, near=False,
        grid=(1,),
        in_specs=[kept(x.shape) for x in tokens] + [upper] * len(blocks),
        out_specs=kept((count, rows * 2 // 3)),
    )


def dense_out_kernel(*refs):
    planes, tps = lax.axis_size(Z), lax.axis_size(TP)
    hiddens, blocks = refs[:tps], refs[tps : tps + planes]
    gate_ref, rows_ref, high_ref, low_ref, home_ref, away_ref = refs[tps + planes :]
    units = blocks[0].shape[0] // tps
    total = 0.0
    for k in range(tps):
        at = span(behind(TP, k), units)
        total = total + dot(
            hiddens[k][...], jnp.concatenate([b[at, :] for b in blocks], axis=0)
        )
    rows = rows_ref[...]
    total = total * gate_ref[:, 0:1] + (dot(high_ref[...], rows) + dot(low_ref[...], rows))
    half = home_ref.shape[0]
    home_ref[...] = total[:half]
    away_ref[...] = total[half:].astype(BF16)


def dense_out(hiddens, blocks, gate, returned, high, low):
    half = hiddens[0].shape[0] // 2
    rows, width = blocks[0].shape
    kept = lambda shape: pl.BlockSpec(shape, lambda i: (0, 0))
    lower = pl.BlockSpec((rows // 3, width), lambda i: (2, 0))
    others = (gate, returned, high, low)
    return call(
        dense_out_kernel,
        (
            jax.ShapeDtypeStruct((half, width), F32),
            jax.ShapeDtypeStruct((half, width), BF16),
        ),
        400_000_000, 2_000_000, *hiddens, *blocks, *others, near=False,
        grid=(1,),
        in_specs=[kept(x.shape) for x in hiddens]
        + [lower] * len(blocks)
        + [kept(x.shape) for x in others],
        out_specs=(kept((half, width)), kept((half, width))),
    )


def fold_kernel(home_ref, come_ref, resid_ref, *outs):
    seq = resid_ref.shape[0]
    total = home_ref[...] + come_ref[...].astype(F32)
    outs[0][...] = resid_ref[...] + total[:seq]
    for j in range(1, len(outs)):
        outs[j][...] = total[j * seq : (j + 1) * seq].astype(BF16)


def fold(home, come, resid):
    keep = jax.ShapeDtypeStruct(resid.shape, F32)
    sent = jax.ShapeDtypeStruct(resid.shape, BF16)
    outs = (keep,) + (sent,) * (lax.axis_size(Y) - 1)
    return call(fold_kernel, outs, 100_000, 500_000, home, come, resid)


def finish_kernel(keep_ref, *refs):
    parts, out_ref = refs[:-1], refs[-1]
    total = keep_ref[...]
    for part in parts:
        total = total + part[...].astype(F32)
    out_ref[...] = total.astype(BF16)


def finish(keep, parts):
    return call(finish_kernel, jax.ShapeDtypeStruct(keep.shape, BF16), 0, 200_000, keep, *parts)


def along_z(own):
    blocks = [own]
    right = left = own
    for _ in range(1, lax.axis_size(Z) // 2 + 1):
        right = shifted(right, Z, 1)
        blocks.append(right)
        if len(blocks) < lax.axis_size(Z):
            left = shifted(left, Z, -1)
            blocks.append(left)
    return blocks


def over_z(rows):
    planes = lax.axis_size(Z)
    shaped = rows.reshape(planes, -1, rows.shape[1])
    return lax.all_to_all(shaped, Z, split_axis=0, concat_axis=0, tiled=True).reshape(rows.shape)


def shards(
    tokens,
    norm_attn,
    w_query,
    w_key,
    w_value,
    w_out,
    head_bias,
    key_cache,
    value_cache,
    lengths,
    norm_ffn,
    w_group,
    w_fine,
    routes,
    e_gate,
    e_up,
    e_down,
    d_gate,
    d_up,
    d_down,
    w_mix,
):
    seq_count = tokens.shape[0]
    width_part = d_gate.shape[0]
    kv_local = key_cache.shape[1]
    head_dim = key_cache.shape[3]
    wide = prepare(d_gate, d_up)
    arrived = [wide[0]] + [shifted(wide[k], TP, k) for k in range(1, len(wide))]
    partial_value, new_keys, new_values = attention(
        tokens,
        norm_attn,
        w_query,
        w_key.T,
        w_value.T,
        w_out,
        head_bias,
        key_cache.transpose(0, 1, 3, 2),
        value_cache.transpose(0, 1, 3, 2),
        lengths,
    )
    parts = all_shifts(partial_value, TP)
    own = jnp.concatenate([*arrived, d_down], axis=0)
    blocks = along_z(own)
    payload, resid = norm_payload(tokens, norm_ffn, routes, parts)
    here = all_shifts(payload, Y)
    group = here + [shifted(x, CORE, 1) for x in here]
    rows, hot = select(group, width_part)
    rows = over_z(rows)
    pre = expert_in(rows, e_gate[0], e_up[0])
    pres = [pre[0]] + [shifted(pre[k], TP, k) for k in range(1, len(pre))]
    act = expert_act(pres)
    acts = all_shifts(act, TP)
    result = expert_out(acts, e_down[0])
    returned = over_z(result)
    high, low, gate = share_weights(hot, w_group, w_fine, w_mix, group)
    hidden = dense_in(group, blocks)
    hiddens = all_shifts(hidden, TP)
    home, away = dense_out(hiddens, blocks, gate, returned, high, low)
    come = shifted(away, CORE, 1)
    folded = fold(home, come, resid)
    parts = [shifted(folded[j], Y, -j) for j in range(1, len(folded))]
    mixed = finish(folded[0], parts)
    return (
        mixed,
        new_keys.reshape(seq_count, kv_local, head_dim),
        new_values.reshape(seq_count, kv_local, head_dim),
    )


def solution(mesh):
    torus = Mesh(mesh.devices.reshape(8, 4, 2, mesh.shape["tp"]), ("ep_0", "ep_1", "ep_2", "tp"))
    placed = (
        P(EP, None),
        P(),
        P(None, "tp"),
        P(None, "tp"),
        P(None, "tp"),
        P("tp", None),
        P("tp"),
        P(EP, "tp", None, None),
        P(EP, "tp", None, None),
        P(EP),
        P(),
        P(),
        P(),
        P(EP, None),
        P(EP, "tp", None),
        P(EP, "tp", None),
        P(EP, None, "tp"),
        P("tp", EP),
        P("tp", EP),
        P(EP, "tp"),
        P(),
    )
    return jax.shard_map(
        shards,
        mesh=torus,
        in_specs=placed,
        out_specs=(P(EP, "tp"), P(EP, "tp", None), P(EP, "tp", None)),
        check_vma=False,
    )
```

```python
import jax
import jax.numpy as jnp
from jax import lax
from jax.experimental import pallas as pl
from jax.experimental.pallas import tpu as pltpu
from jax.sharding import Mesh
from jax.sharding import PartitionSpec as P


EP = ("ep_0", "ep_1", "ep_2")
Z, Y, CORE, TP = "ep_0", "ep_1", "ep_2", "tp"

norm_eps = 1e-06
PIECE = 128
CHUNK = 8
EXTRA = 128
SLOTS = 16
VMEM_LIMIT = 12 * 2**20
NT = (((1,), (1,)), ((), ()))
F32 = jnp.float32
BF16 = jnp.bfloat16


def shifted(x, axis, step):
    size = lax.axis_size(axis)
    return lax.ppermute(x, axis, [(i, (i + step) % size) for i in range(size)])


def all_shifts(x, axis):
    return [x] + [shifted(x, axis, k) for k in range(1, lax.axis_size(axis))]


def silu(v):
    return v / (1.0 + jnp.exp(-v))


def dot(a, b):
    return jnp.dot(a, b, preferred_element_type=F32)


def dot_nt(a, b):
    return lax.dot_general(a, b, NT, preferred_element_type=F32)


def behind(axis, k):
    size = lax.axis_size(axis)
    return lax.rem(lax.axis_index(axis) - k + size, size)


def span(index, size):
    return pl.ds(pl.multiple_of(index * size, size), size)


def call(kernel, out, flops, moved, *operands, near=True, **more):
    if near:
        more["compiler_params"] = pltpu.CompilerParams(vmem_limit_bytes=VMEM_LIMIT)
    return pl.pallas_call(
        kernel,
        out_shape=out,
        cost_estimate=pl.CostEstimate(flops=flops, bytes_accessed=moved, transcendentals=0),
        **more,
    )(*operands)


def attention_kernel(
    lengths_ref, tokens_ref, gain_ref, bias_ref, wk_ref, wv_ref,
    wq_hbm, keys_hbm, values_hbm, wo_hbm,
    partial_ref, new_keys_ref, new_values_ref,
    wq_ref, keys_ref, values_ref, wo_ref,
    q_ref, split_ref, reach_ref, stop_ref, mixed_ref, heads_ref, sems,
):
    seq, heads, dim = q_ref.shape
    length = keys_ref.shape[2]
    pieces = length // PIECE
    chunks = seq // CHUNK

    def fetch(source, target, number):
        return pltpu.make_async_copy(source, target, sems.at[number])

    query_copy = fetch(wq_hbm, wq_ref, 0)
    key_copies = [
        fetch(keys_hbm.at[pl.ds(c * CHUNK, CHUNK)], keys_ref.at[pl.ds(c * CHUNK, CHUNK)], 2 + c)
        for c in range(chunks)
    ]
    value_copies = [
        fetch(
            values_hbm.at[pl.ds(c * CHUNK, CHUNK)],
            values_ref.at[pl.ds(c * CHUNK, CHUNK)],
            2 + chunks + c,
        )
        for c in range(chunks)
    ]
    out_copy = fetch(wo_hbm, wo_ref, 1)
    query_copy.start()
    for c in range(chunks):
        key_copies[c].start()
        value_copies[c].start()
    out_copy.start()

    wide = tokens_ref[...].astype(jnp.float32)
    scale = lax.rsqrt(jnp.mean(wide * wide, axis=-1, keepdims=True) + norm_eps)
    h_first = (wide * scale * gain_ref[...]).astype(jnp.bfloat16)
    for weight, target in ((wk_ref, new_keys_ref), (wv_ref, new_values_ref)):
        target[...] = lax.dot_general(
            h_first, weight[...], NT, preferred_element_type=jnp.float32
        ).astype(jnp.bfloat16)
    query_copy.wait()
    queries = jnp.dot(h_first, wq_ref[...], preferred_element_type=jnp.float32)
    for g in range(heads):
        q_ref[:, g, :] = queries[:, g * dim : (g + 1) * dim]

    row = lax.broadcasted_iota(jnp.int32, (2 * PIECE, 2 * PIECE), 0) % PIECE
    column = lax.broadcasted_iota(jnp.int32, (2 * PIECE, 2 * PIECE), 1)
    later = ((row > column) | (column >= PIECE)).astype(jnp.bfloat16)
    position = lax.broadcasted_iota(jnp.int32, (heads, PIECE), 1)
    head = lax.broadcasted_iota(jnp.int32, (heads, PIECE), 0)
    bias = jnp.full((heads, PIECE), bias_ref[0], jnp.float32)
    for g in range(1, heads):
        bias = jnp.where(head == g, bias_ref[g], bias)

    for c in range(chunks):
        key_copies[c].wait()
        for i in range(CHUNK):
            b = c * CHUNK + i
            scores = jnp.dot(
                q_ref[b].astype(jnp.bfloat16), keys_ref[b], preferred_element_type=jnp.float32
            )
            for p in range(pieces):
                s = scores[:, p * PIECE : (p + 1) * PIECE] * dim ** (-0.5) + bias
                inside = position < lengths_ref[b] - p * PIECE
                rest = jnp.log(1.0 + jnp.exp(-jnp.abs(s)))
                fail = jnp.where(inside, -(jnp.maximum(s, 0.0) + rest), 0.0)
                stop_ref[i, p] = jnp.where(inside, jnp.minimum(s, 0.0) - rest, -jnp.inf)
                high = fail.astype(jnp.bfloat16)
                low = (fail - high.astype(jnp.float32)).astype(jnp.bfloat16)
                at = (i * pieces + p) * heads
                split_ref[at : at + heads, :PIECE] = high.astype(jnp.float32)
                split_ref[at : at + heads, PIECE:] = low.astype(jnp.float32)
        reach_ref[...] = jnp.dot(
            split_ref[...].astype(jnp.bfloat16), later, preferred_element_type=jnp.float32
        )
        value_copies[c].wait()
        for i in range(CHUNK):
            b = c * CHUNK + i
            carried = None
            weights = [None] * pieces
            for p in reversed(range(pieces)):
                at = (i * pieces + p) * heads
                within = reach_ref[at : at + heads, :PIECE]
                whole = reach_ref[at : at + heads, PIECE:]
                exponent = stop_ref[i, p] + within
                if carried is not None:
                    exponent = exponent + carried
                weights[p] = jnp.exp(exponent)
                carried = whole if carried is None else carried + whole
            stick = jnp.concatenate(weights, axis=1).astype(jnp.bfloat16)
            mixed_ref[b] = lax.dot_general(
                stick, values_ref[b], NT, preferred_element_type=jnp.float32
            )
    for g in range(heads):
        heads_ref[:, g * dim : (g + 1) * dim] = mixed_ref[:, g, :]
    out_copy.wait()
    partial_ref[...] = jnp.dot(
        heads_ref[...].astype(jnp.bfloat16), wo_ref[...], preferred_element_type=jnp.float32
    ).astype(jnp.bfloat16)


def attention(tokens, gain, wq, wk, wv, wo, bias, keys, values, lengths):
    seq, width = tokens.shape
    dim, length = keys.shape[2], keys.shape[3]
    heads = bias.shape[0]
    keys, values = keys[:, 0], values[:, 0]
    pieces = length // PIECE
    rows = CHUNK * pieces * heads
    vmem = pl.BlockSpec(memory_space=pltpu.VMEM)
    anywhere = pl.BlockSpec(memory_space=pltpu.HBM)
    smem = pl.BlockSpec(memory_space=pltpu.SMEM)
    return pl.pallas_call(
        attention_kernel,
        out_shape=(
            jax.ShapeDtypeStruct((seq, width), jnp.bfloat16),
            jax.ShapeDtypeStruct((seq, dim), jnp.bfloat16),
            jax.ShapeDtypeStruct((seq, dim), jnp.bfloat16),
        ),
        in_specs=[smem, vmem, vmem, smem, vmem, vmem] + [anywhere] * 4,
        out_specs=(vmem, vmem, vmem),
        scratch_shapes=[
            pltpu.VMEM(wq.shape, jnp.bfloat16),
            pltpu.VMEM(keys.shape, jnp.bfloat16),
            pltpu.VMEM(values.shape, jnp.bfloat16),
            pltpu.VMEM(wo.shape, jnp.bfloat16),
            pltpu.VMEM((seq, heads, dim), jnp.float32),
            pltpu.VMEM((rows, 2 * PIECE), jnp.float32),
            pltpu.VMEM((rows, 2 * PIECE), jnp.float32),
            pltpu.VMEM((CHUNK, pieces, heads, PIECE), jnp.float32),
            pltpu.VMEM((seq, heads, dim), jnp.float32),
            pltpu.VMEM((seq, heads * dim), jnp.float32),
            pltpu.SemaphoreType.DMA((2 + 2 * (seq // CHUNK),)),
        ],
        cost_estimate=pl.CostEstimate(
            flops=400_000_000, bytes_accessed=11_000_000, transcendentals=600_000
        ),
        name="attention",
    )(lengths, tokens, gain[None, :], bias, wk, wv, wq, keys, values, wo)


def prepare_kernel(gate_ref, up_ref, *outs_and_scratch):
    outs, (gates, ups) = outs_and_scratch[:-2], outs_and_scratch[-2:]
    units = outs[0].shape[0] // 2
    gates[...] = gate_ref[...].T
    ups[...] = up_ref[...].T
    for k, out in enumerate(outs):
        at = span(behind(TP, -k), units)
        out[:units, :] = gates[at, :]
        out[units:, :] = ups[at, :]


def prepare(d_gate, d_up):
    tps = lax.axis_size(TP)
    width, units = d_gate.shape
    one = jax.ShapeDtypeStruct((2 * units // tps, width), BF16)
    turned = pltpu.VMEM((units, width), BF16)
    return call(
        prepare_kernel, (one,) * tps, 0, 600_000, d_gate, d_up,
        scratch_shapes=[turned, turned],
    )


def norm_kernel(tokens_ref, gain_ref, routes_ref, *refs):
    parts, (payload_ref, slice_ref, resid_ref) = refs[:-3], refs[-3:]
    seq, width = tokens_ref.shape
    attended = parts[0][...].astype(F32)
    for part in parts[1:]:
        attended = attended + part[...].astype(F32)
    resid = tokens_ref[...].astype(F32) + attended
    resid_ref[...] = resid
    scale = lax.rsqrt(jnp.mean(resid * resid, axis=-1, keepdims=True) + norm_eps)
    payload_ref[:, :width] = (resid * scale * gain_ref[...]).astype(BF16)
    lane = lax.broadcasted_iota(jnp.int32, (seq, EXTRA), 1)
    routes = routes_ref[...]
    named = jnp.where(lane == 0, routes[:, 0:1], jnp.where(lane == 1, routes[:, 1:2], 0))
    payload_ref[:, width:] = named.astype(F32).astype(BF16)
    slice_ref[...] = resid_ref[:, span(lax.axis_index(TP), slice_ref.shape[1])]


def norm_payload(tokens, gain, routes, parts):
    seq, width = tokens.shape
    return call(
        norm_kernel,
        (
            jax.ShapeDtypeStruct((seq, width + EXTRA), BF16),
            jax.ShapeDtypeStruct((seq, width // lax.axis_size(TP)), F32),
        ),
        1_000_000, 600_000, tokens, gain[None, :], routes, *parts,
        scratch_shapes=[pltpu.VMEM((seq, width), F32)],
    )


def group_routes(tokens):
    width = tokens[0].shape[1] - EXTRA
    extra = jnp.concatenate([ref[:, width:].astype(F32) for ref in tokens], axis=0)
    first, second = extra[:, 0:1], extra[:, 1:2]
    slots = lax.axis_size(Z) * SLOTS
    lane = lax.broadcasted_iota(jnp.int32, (extra.shape[0], slots), 1)
    plane = lax.axis_size(Y) * lax.axis_size(CORE)
    place = lax.axis_index(Y) * lax.axis_size(CORE) + lax.axis_index(CORE)
    expert = ((lane // SLOTS) * plane + place).astype(F32)
    return first, second, expert, (lane % SLOTS).astype(F32)


def select_kernel(*refs):
    tokens, (rows_ref, hot_ref) = refs[:-2], refs[-2:]
    part = rows_ref.shape[1]
    first, second, expert, slot = group_routes(tokens)
    match = ((first == expert) | (second == expert)).astype(F32)
    count = match.shape[0]
    row = lax.broadcasted_iota(jnp.int32, (count, count), 0)
    column = lax.broadcasted_iota(jnp.int32, (count, count), 1)
    rank = dot((column < row).astype(BF16), match.astype(BF16))
    hot = jnp.where(rank == slot, match, 0.0)
    hot_ref[...] = hot.astype(BF16)
    mine = jnp.concatenate(
        [ref[:, span(lax.axis_index(TP), part)].astype(F32) for ref in tokens], axis=0
    ).astype(BF16)
    rows_ref[...] = dot(hot.T.astype(BF16), mine).astype(BF16)


def select(tokens, part):
    slots = lax.axis_size(Z) * SLOTS
    count = len(tokens) * tokens[0].shape[0]
    return call(
        select_kernel,
        (
            jax.ShapeDtypeStruct((slots, part), BF16),
            jax.ShapeDtypeStruct((count, slots), BF16),
        ),
        40_000_000, 1_000_000, *tokens,
    )


def share_kernel(hot_ref, group_ref, fine_ref, mix_ref, *refs):
    tokens, (high_ref, low_ref, gate_ref) = refs[:-3], refs[-3:]
    width = group_ref.shape[1]
    per_group = fine_ref.shape[0] // group_ref.shape[0]
    rows = jnp.concatenate([ref[:, :width].astype(F32) for ref in tokens], axis=0)
    narrow = rows.astype(BF16)
    group_logits = dot_nt(narrow, group_ref[...])
    fine_logits = dot_nt(narrow, fine_ref[...])
    first, second, expert, _ = group_routes(tokens)
    group = lax.broadcasted_iota(jnp.int32, group_logits.shape, 1)
    own = (first.astype(jnp.int32) // per_group) == group
    own_logit = jnp.sum(jnp.where(own, group_logits, 0.0), axis=1, keepdims=True)
    group_share = 1.0 / jnp.sum(jnp.exp(group_logits - own_logit), axis=1, keepdims=True)
    fine = lax.broadcasted_iota(jnp.int32, fine_logits.shape, 1).astype(F32)
    picked = [
        jnp.sum(jnp.where(fine == chosen, fine_logits, 0.0), axis=1, keepdims=True)
        for chosen in (first, second)
    ]
    weight = 0.0
    for chosen, here, there in ((first, 0, 1), (second, 1, 0)):
        share = group_share * (1.0 / (1.0 + jnp.exp(picked[there] - picked[here])))
        weight = weight + jnp.where(chosen == expert, share, 0.0)
    weight = weight * hot_ref[...].astype(F32)
    high = weight.astype(BF16)
    high_ref[...] = high
    low_ref[...] = (weight - high.astype(F32)).astype(BF16)
    mix = jnp.sum(rows * mix_ref[...], axis=1, keepdims=True)
    gate_ref[...] = jnp.broadcast_to(1.0 / (1.0 + jnp.exp(-mix)), gate_ref.shape)


def share_weights(hot, w_group, w_fine, w_mix, tokens):
    table = jax.ShapeDtypeStruct(hot.shape, BF16)
    return call(
        share_kernel,
        (table, table, jax.ShapeDtypeStruct((hot.shape[0], EXTRA), F32)),
        60_000_000, 1_500_000, hot, w_group.T, w_fine.T, w_mix[None, :], *tokens, near=False,
    )


def expert_in_kernel(rows_ref, gate_ref, up_ref, *outs):
    units = outs[0].shape[1] // 2
    rows = rows_ref[...]
    for k, out in enumerate(outs):
        at = span(behind(TP, -k), units)
        both = jnp.concatenate([gate_ref[:, at], up_ref[:, at]], axis=1)
        out[...] = dot(rows, both).astype(BF16)


def expert_in(rows, gate, up):
    tps = lax.axis_size(TP)
    one = jax.ShapeDtypeStruct((rows.shape[0], 2 * gate.shape[1] // tps), BF16)
    return call(expert_in_kernel, (one,) * tps, 140_000_000, 1_400_000, rows, gate, up)


def expert_act_kernel(*refs):
    parts, out_ref = refs[:-1], refs[-1]
    units = out_ref.shape[1]
    act = parts[0][...].astype(F32)
    for part in parts[1:]:
        act = act + part[...].astype(F32)
    out_ref[...] = (silu(act[:, :units]) * act[:, units:]).astype(BF16)


def expert_act(parts):
    rows, width = parts[0].shape
    return call(
        expert_act_kernel,
        jax.ShapeDtypeStruct((rows, width // 2), BF16),
        1_000_000, 300_000, *parts,
    )


def expert_out_kernel(*refs):
    hiddens, (down_ref, out_ref, hidden_ref) = refs[:-3], refs[-3:]
    for k, hidden in enumerate(hiddens):
        hidden_ref[:, span(behind(TP, k), hidden.shape[1])] = hidden[...]
    out_ref[...] = dot(hidden_ref[...], down_ref[...]).astype(BF16)


def expert_out(hiddens, down):
    return call(
        expert_out_kernel,
        jax.ShapeDtypeStruct((hiddens[0].shape[0], down.shape[1]), BF16),
        70_000_000, 800_000, *hiddens, down,
        scratch_shapes=[pltpu.VMEM((hiddens[0].shape[0], down.shape[0]), BF16)],
    )


def dense_in_kernel(*refs):
    out_ref = refs[-1]
    planes, tps = lax.axis_size(Z), lax.axis_size(TP)
    tokens, blocks = refs[: -planes - 1], refs[-planes - 1 : -1]
    width = blocks[0].shape[1]
    units = out_ref.shape[1] // planes
    gate = up = 0.0
    for k in range(tps):
        at = span(behind(TP, k), width)
        rows = jnp.concatenate([ref[:, at].astype(F32) for ref in tokens], axis=0).astype(BF16)
        low, mid, top = 2 * k * units, (2 * k + 1) * units, (2 * k + 2) * units
        gate = gate + dot_nt(rows, jnp.concatenate([b[low:mid, :] for b in blocks], axis=0))
        up = up + dot_nt(rows, jnp.concatenate([b[mid:top, :] for b in blocks], axis=0))
    out_ref[...] = (silu(gate) * up).astype(BF16)


def dense_in(tokens, blocks):
    count = len(tokens) * tokens[0].shape[0]
    rows, width = blocks[0].shape
    whole = pl.BlockSpec(memory_space=pltpu.VMEM)
    upper = pl.BlockSpec((rows * 2 // 3, width), lambda i: (0, 0))
    kept = lambda shape: pl.BlockSpec(shape, lambda i: (0, 0))
    return call(
        dense_in_kernel,
        jax.ShapeDtypeStruct((count, rows * 2 // 3), BF16),
        400_000_000, 3_000_000, *tokens, *blocks, near=False,
        grid=(1,),
        in_specs=[kept(x.shape) for x in tokens] + [upper] * len(blocks),
        out_specs=kept((count, rows * 2 // 3)),
    )


def dense_out_kernel(*refs):
    planes, tps = lax.axis_size(Z), lax.axis_size(TP)
    hiddens, blocks = refs[:tps], refs[tps : tps + planes]
    gate_ref, rows_ref, high_ref, low_ref, home_ref, away_ref = refs[tps + planes :]
    units = blocks[0].shape[0] // tps
    total = 0.0
    for k in range(tps):
        at = span(behind(TP, k), units)
        total = total + dot(
            hiddens[k][...], jnp.concatenate([b[at, :] for b in blocks], axis=0)
        )
    rows = rows_ref[...]
    total = total * gate_ref[:, 0:1] + (dot(high_ref[...], rows) + dot(low_ref[...], rows))
    half = home_ref.shape[0]
    home_ref[...] = total[:half]
    away_ref[...] = total[half:].astype(BF16)


def dense_out(hiddens, blocks, gate, returned, high, low):
    half = hiddens[0].shape[0] // 2
    rows, width = blocks[0].shape
    kept = lambda shape: pl.BlockSpec(shape, lambda i: (0, 0))
    lower = pl.BlockSpec((rows // 3, width), lambda i: (2, 0))
    others = (gate, returned, high, low)
    return call(
        dense_out_kernel,
        (
            jax.ShapeDtypeStruct((half, width), F32),
            jax.ShapeDtypeStruct((half, width), BF16),
        ),
        400_000_000, 2_000_000, *hiddens, *blocks, *others, near=False,
        grid=(1,),
        in_specs=[kept(x.shape) for x in hiddens]
        + [lower] * len(blocks)
        + [kept(x.shape) for x in others],
        out_specs=(kept((half, width)), kept((half, width))),
    )


def fold_kernel(home_ref, come_ref, resid_ref, *outs):
    seq = resid_ref.shape[0]
    total = home_ref[...] + come_ref[...].astype(F32)
    outs[0][...] = resid_ref[...] + total[:seq]
    for j in range(1, len(outs)):
        outs[j][...] = total[j * seq : (j + 1) * seq].astype(BF16)


def fold(home, come, resid):
    keep = jax.ShapeDtypeStruct(resid.shape, F32)
    sent = jax.ShapeDtypeStruct(resid.shape, BF16)
    outs = (keep,) + (sent,) * (lax.axis_size(Y) - 1)
    return call(fold_kernel, outs, 100_000, 500_000, home, come, resid)


def finish_kernel(keep_ref, *refs):
    parts, out_ref = refs[:-1], refs[-1]
    total = keep_ref[...]
    for part in parts:
        total = total + part[...].astype(F32)
    out_ref[...] = total.astype(BF16)


def finish(keep, parts):
    return call(finish_kernel, jax.ShapeDtypeStruct(keep.shape, BF16), 0, 200_000, keep, *parts)


def along_z(own):
    blocks = [own]
    right = left = own
    for _ in range(1, lax.axis_size(Z) // 2 + 1):
        right = shifted(right, Z, 1)
        blocks.append(right)
        if len(blocks) < lax.axis_size(Z):
            left = shifted(left, Z, -1)
            blocks.append(left)
    return blocks


def over_z(rows):
    planes = lax.axis_size(Z)
    shaped = rows.reshape(planes, -1, rows.shape[1])
    return lax.all_to_all(shaped, Z, split_axis=0, concat_axis=0, tiled=True).reshape(rows.shape)


def shards(
    tokens,
    norm_attn,
    w_query,
    w_key,
    w_value,
    w_out,
    head_bias,
    key_cache,
    value_cache,
    lengths,
    norm_ffn,
    w_group,
    w_fine,
    routes,
    e_gate,
    e_up,
    e_down,
    d_gate,
    d_up,
    d_down,
    w_mix,
):
    seq_count = tokens.shape[0]
    width_part = d_gate.shape[0]
    kv_local = key_cache.shape[1]
    head_dim = key_cache.shape[3]
    wide = prepare(d_gate, d_up)
    arrived = [wide[0]] + [shifted(wide[k], TP, k) for k in range(1, len(wide))]
    partial_value, new_keys, new_values = attention(
        tokens,
        norm_attn,
        w_query,
        w_key.T,
        w_value.T,
        w_out,
        head_bias,
        key_cache.transpose(0, 1, 3, 2),
        value_cache.transpose(0, 1, 3, 2),
        lengths,
    )
    parts = all_shifts(partial_value, TP)
    own = jnp.concatenate([*arrived, d_down], axis=0)
    blocks = along_z(own)
    payload, resid = norm_payload(tokens, norm_ffn, routes, parts)
    here = all_shifts(payload, Y)
    group = here + [shifted(x, CORE, 1) for x in here]
    rows, hot = select(group, width_part)
    rows = over_z(rows)
    pre = expert_in(rows, e_gate[0], e_up[0])
    pres = [pre[0]] + [shifted(pre[k], TP, k) for k in range(1, len(pre))]
    act = expert_act(pres)
    acts = all_shifts(act, TP)
    result = expert_out(acts, e_down[0])
    returned = over_z(result)
    high, low, gate = share_weights(hot, w_group, w_fine, w_mix, group)
    hidden = dense_in(group, blocks)
    hiddens = all_shifts(hidden, TP)
    home, away = dense_out(hiddens, blocks, gate, returned, high, low)
    come = shifted(away, CORE, 1)
    folded = fold(home, come, resid)
    parts = [shifted(folded[j], Y, -j) for j in range(1, len(folded))]
    mixed = finish(folded[0], parts)
    return (
        mixed,
        new_keys.reshape(seq_count, kv_local, head_dim),
        new_values.reshape(seq_count, kv_local, head_dim),
    )


def solution(mesh):
    torus = Mesh(mesh.devices.reshape(8, 4, 2, mesh.shape["tp"]), ("ep_0", "ep_1", "ep_2", "tp"))
    placed = (
        P(EP, None),
        P(),
        P(None, "tp"),
        P(None, "tp"),
        P(None, "tp"),
        P("tp", None),
        P("tp"),
        P(EP, "tp", None, None),
        P(EP, "tp", None, None),
        P(EP),
        P(),
        P(),
        P(),
        P(EP, None),
        P(EP, "tp", None),
        P(EP, "tp", None),
        P(EP, None, "tp"),
        P("tp", EP),
        P("tp", EP),
        P(EP, "tp"),
        P(),
    )
    return jax.shard_map(
        shards,
        mesh=torus,
        in_specs=placed,
        out_specs=(P(EP, "tp"), P(EP, "tp", None), P(EP, "tp", None)),
        check_vma=False,
    )
```
